256 devices in a mesh: grp: 2 (over y), sp: 32 (over z, core), tp: 4 (over x).
Axes of the slice: x: 4, y: 2, z: 16, core: 2. Of those that a mesh axis runs over, the one named last changes fastest.
The devices are a block of a 4x16x16 slice.
Arguments:
- queries: bfloat16 [16384, 512], P(('grp', 'sp'), 'tp'), parts along dimension 0, may hold values from -6 to 6
- key_rows: bfloat16 [16384, 512], P(('grp', 'sp'), 'tp'), parts along dimension 0, may hold values from -6 to 6
- value_rows: bfloat16 [16384, 1024], P(('grp', 'sp'), 'tp'), parts along dimension 0, may hold values from -6 to 6
- out_gate: bfloat16 [16384, 1024], P(('grp', 'sp'), 'tp'), parts along dimension 0, may hold values from -6 to 6
- log_decay: float32 [2, 16384, 512], P(None, ('grp', 'sp'), 'tp'), parts along dimension 1
- doc_ids: int32 [16384], P(('grp', 'sp')), parts along dimension 0, may hold values from 0 to 3, as said below
- head_gain: float32 [1024], P('tp'), may hold values from 0.1 to 1.9
- out_weight: bfloat16 [1024, 2048], P('tp'), may hold values from -0.375 to 0.375
- residual: bfloat16 [16384, 2048], P(('grp', 'sp'), 'tp'), parts along dimension 0
- norm_gain: float32 [2, 2048], replicated, may hold values from 0.1 to 1.9
- norm_bias: float32 [2, 2048], replicated, may hold values from -3 to 3
- gate_weight: bfloat16 [2048, 3072], P('sp', 'tp'), may hold values from -0.125 to 0.125
- up_weight: bfloat16 [2048, 3072], P('sp', 'tp'), may hold values from -0.125 to 0.125
- down_weight: bfloat16 [3072, 2048], P('tp', 'sp'), may hold values from -0.109375 to 0.109375
Outputs:
- layer_out: bfloat16 [16384, 2048], P(('grp', 'sp'), 'tp'), parts along dimension 0
The draws below stay inside these ranges and needn't reach their ends.
There are 2 independent parts, one for each index of `grp`. The reference program is written for one: setup_inputs(seed, part) draws one part's arguments, and reference() takes and returns one part's arrays. A program takes and returns all parts, laid end to end along the dimension named above; an argument that names none is the same for every part. Nothing has to cross between parts.
Inputs may be any that keep to these rules, and one draw needn't show every extreme that they name: `doc_ids`: document numbers start at 0 and never fall; they rise by one at each of 3 positions, the k-th rise lying within half of 256 positions of k times 8192 divided by 4.
All inputs are finite; a program needn't handle non-finite values.
Results may differ from the reference program's by a relative error of at most 0.009.
Values may be sent and summed in bfloat16 or wider, within the bound.
No kernel may reach another device: no remote copies, remote signals or barrier semaphores. Data moves between devices by JAX's collectives and lax.ppermute only.
A program may use at most 128 MiB of HBM per device.

```python
import math
import jax
import jax.numpy as jnp
from jax import lax

D = 2048
HEADS = 16
DK = 32
DV = 64
FF = 3072
BLOCK = 64
TOK_DEV = 256
SEQ = 8192
DOCS = 4
KW = 512
GW = 1024
N_TP = 4


def draw_log_decay(key, part):
    streams = jax.random.split(key, 6)
    fast_share = 0.5
    fast = jax.random.uniform(streams[0], (2, 1, KW)) < fast_share
    decay_speed = jnp.where(fast, 1.0 / 40.0, 0.5 * DOCS / SEQ)
    reach_multiplier = jnp.exp(jax.random.uniform(streams[1], (2, SEQ // TOK_DEV, 1), minval=-0.9, maxval=0.9))
    reach_multiplier = jnp.repeat(reach_multiplier, TOK_DEV, axis=1)
    block_multiplier = jnp.exp(jax.random.uniform(streams[2], (2, SEQ // BLOCK, 1), minval=-0.35, maxval=0.35))
    block_multiplier = jnp.repeat(block_multiplier, BLOCK, axis=1)
    random_perturbation = jnp.exp(0.5 * jax.random.normal(streams[3], (2, SEQ, KW)))
    marked_locations = jax.random.randint(streams[4], (2, 8, 1), 0, SEQ)
    layer_depth_count = jnp.log(jax.random.uniform(streams[5], (2, 8, 1), minval=0.5, maxval=0.8))
    token_location = jnp.arange(SEQ, dtype=jnp.int32)[None, None, :]
    spike_amplitude = jnp.sum(jnp.where(marked_locations == token_location, layer_depth_count, 0.0), axis=1)
    return (-decay_speed * reach_multiplier * block_multiplier * random_perturbation + spike_amplitude[:, :, None]).astype(jnp.float32)


def draw_doc_ids(key, part):
    shifts = jax.random.randint(key, (DOCS - 1,), -(TOK_DEV // 2), TOK_DEV // 2 + 1)
    cuts = jnp.arange(1, DOCS, dtype=jnp.int32) * (SEQ // DOCS) + shifts
    token_location = jnp.arange(SEQ, dtype=jnp.int32)
    return jnp.sum((token_location[:, None] >= cuts[None, :]).astype(jnp.int32), axis=1)


def draw_residual(key, part):
    streams = jax.random.split(key, 3)
    base = jax.random.normal(streams[0], (SEQ, D))
    rising = 3.0 ** (jnp.arange(D, dtype=jnp.float32) / (D - 1))
    rising = rising * jnp.exp(jax.random.uniform(streams[1], (D,), minval=-0.4, maxval=0.4))
    row_scale = jnp.exp(jax.random.uniform(streams[2], (SEQ, 1), minval=math.log(0.5), maxval=math.log(5.0)))
    return (base * rising * row_scale).astype(jnp.bfloat16)


def steps_of(stream_key, shape, cuts, least, high):
    def one(position, parts):
        steps = jax.random.uniform(jax.random.fold_in(jax.random.fold_in(stream_key, 6), position), (parts,), jnp.float32, least / len(cuts), high / len(cuts))
        return jnp.repeat(jnp.exp(steps), shape[position] // parts).reshape((-1,) + (1,) * (len(shape) - position - 1))

    factor_of = one(*cuts[0])
    for cut in cuts[1:]:
        factor_of = factor_of * one(*cut)
    return factor_of


def bell_draw(own_key, shape, width, reach, pieces=(), kind=jnp.bfloat16):
    loudness = steps_of(own_key, shape, pieces, -0.22, 0.18) if pieces else 1.0
    drawn = jax.random.normal(own_key, shape, jnp.float32) * width * loudness
    return jnp.minimum(jnp.maximum(drawn, -reach), reach).astype(kind)


def setup_inputs(seed: int = 0, part: int = 0) -> dict:
    key_list = jax.random.split(jax.random.key(seed), 15)
    part_splits = jax.random.split(jax.random.fold_in(key_list[14], part), 15)
    return {
        "queries": bell_draw(part_splits[0], (SEQ, KW), 1.0, 6.0, ((0, 32), (1, 4))),
        "key_rows": bell_draw(part_splits[1], (SEQ, KW), 1.0, 6.0, ((0, 32), (1, 4))),
        "value_rows": bell_draw(part_splits[2], (SEQ, GW), 1.0, 6.0, ((0, 32), (1, 4))),
        "out_gate": bell_draw(part_splits[3], (SEQ, GW), 1.0, 6.0, ((0, 32), (1, 4))),
        "log_decay": draw_log_decay(jax.random.fold_in(jax.random.fold_in(key_list[14], part), 71), part),
        "doc_ids": draw_doc_ids(jax.random.fold_in(jax.random.fold_in(key_list[14], part), 71), part),
        "head_gain": jnp.clip(1.0 + 0.18 * jax.random.normal(key_list[6], (GW,), jnp.float32), 0.1, 1.9),
        "out_weight": bell_draw(key_list[7], (GW, D), (GW // 4) ** -0.5, 0.375, ((0, 4),)),
        "residual": draw_residual(jax.random.fold_in(jax.random.fold_in(key_list[14], part), 71), part),
        "norm_gain": jnp.clip(1.0 + 0.18 * jax.random.normal(key_list[9], (2, D), jnp.float32), 0.1, 1.9),
        "norm_bias": bell_draw(key_list[10], (2, D), 0.5, 3.0, (), jnp.float32),
        "gate_weight": bell_draw(key_list[11], (D, FF), D ** -0.5, 0.125, ((0, 32), (1, 4))),
        "up_weight": bell_draw(key_list[12], (D, FF), D ** -0.5, 0.125, ((0, 32), (1, 4))),
        "down_weight": bell_draw(key_list[13], (FF, D), FF ** -0.5, 0.109375, ((0, 4), (1, 32))),
    }


EPS = 1e-06
HIGH = lax.Precision.HIGHEST

def run_blocks(query, key_part, value_part, decay, docs):
    length = query.shape[0]
    count = length // BLOCK
    head_count = query.shape[1]
    lower = jnp.arange(BLOCK)[:, None] >= jnp.arange(BLOCK)[None, :]

    def blocked(array):
        return array.reshape((count, BLOCK) + array.shape[1:])

    def advance(carried, inputs):
        state, state_doc = carried
        query_block, key_block, value_block, decay_block, doc_block = inputs
        running = jnp.cumsum(decay_block, axis=0)
        allowed = lower & (doc_block[:, None] == doc_block[None, :])
        relative = jnp.exp(jnp.where(allowed[:, :, None, None], running[:, None] - running[None, :], -jnp.inf))
        scores = jnp.einsum('ihd,jhd,ijhd->hij', query_block, key_block, relative, precision=HIGH)
        within = jnp.einsum('hij,jhe->ihe', scores, value_block, precision=HIGH)
        linked = (doc_block == state_doc).astype(query.dtype)
        carried_part = jnp.einsum('ihd,hde->ihe', query_block * jnp.exp(running), state, precision=HIGH) * linked[:, None, None]
        closing = doc_block[-1]
        ending = (doc_block == closing).astype(query.dtype)
        tail_decay = jnp.exp(running[-1][None] - running) * ending[:, None, None]
        kept = (state_doc == closing).astype(query.dtype)
        state = kept * jnp.exp(running[-1])[:, :, None] * state + jnp.einsum('jhd,jhe->hde', key_block * tail_decay, value_block, precision=HIGH)
        return ((state, closing), within + carried_part)
    start = (jnp.zeros((head_count, query.shape[2], value_part.shape[2]), jnp.float32), jnp.array(-1, jnp.int32))
    (state, closing), outputs = lax.scan(advance, start, tuple((blocked(array) for array in (query, key_part, value_part, decay, docs))))
    return (outputs.reshape(length, head_count, value_part.shape[2]), state, closing)

def layer_norm(stream, gain, bias):
    middle = lax.optimization_barrier(jnp.mean(stream, axis=-1, keepdims=True))
    spread = lax.optimization_barrier(jnp.mean(jnp.square(stream - middle), axis=-1, keepdims=True))
    return (stream - middle) * lax.rsqrt(spread + EPS) * gain + bias

def group_sum(left, right):
    group_width = left.shape[1] // N_TP
    summed = jnp.zeros((left.shape[0], right.shape[1]), jnp.float32)
    for group in range(N_TP):
        term = jnp.dot(left[:, group * group_width:(group + 1) * group_width], right[group * group_width:(group + 1) * group_width], preferred_element_type=jnp.float32)
        summed = summed + lax.optimization_barrier(term.astype(jnp.bfloat16)).astype(jnp.float32)
    return summed

def reference(queries, key_rows, value_rows, out_gate, log_decay, doc_ids, head_gain, out_weight, residual, norm_gain, norm_bias, gate_weight, up_weight, down_weight):
    length = queries.shape[0]
    query = queries.astype(jnp.float32).reshape(length, HEADS, DK) * DK ** (-0.5)
    key_part = key_rows.astype(jnp.float32).reshape(length, HEADS, DK)
    value_part = value_rows.astype(jnp.float32).reshape(length, HEADS, DV)
    forward_decay = log_decay[0].reshape(length, HEADS, DK)
    backward_decay = log_decay[1].reshape(length, HEADS, DK)
    forward_out = run_blocks(query, key_part, value_part, forward_decay, doc_ids)[0]
    backward_out = run_blocks(query[::-1], key_part[::-1], value_part[::-1], backward_decay[::-1], doc_ids[::-1])[0][::-1]
    attended = forward_out + backward_out
    normed = attended * lax.rsqrt(lax.optimization_barrier(jnp.mean(attended * attended, axis=-1, keepdims=True)) + EPS)
    mixed = (normed.reshape(length, GW) * head_gain * jax.nn.silu(out_gate.astype(jnp.float32))).astype(jnp.bfloat16)
    branch = group_sum(mixed, out_weight)
    settled = layer_norm(residual.astype(jnp.float32) + branch, norm_gain[0], norm_bias[0])
    features = settled.astype(jnp.bfloat16)
    gate = jnp.dot(features, gate_weight, preferred_element_type=jnp.float32)
    up_part = jnp.dot(features, up_weight, preferred_element_type=jnp.float32)
    inner = (jax.nn.silu(gate) * up_part).astype(jnp.bfloat16)
    down = group_sum(inner, down_weight)
    return layer_norm(settled + 0.5 * down, norm_gain[1], norm_bias[1]).astype(jnp.bfloat16)
```

```python
import functools
import jax
import jax.numpy as jnp
from jax import lax
from jax.experimental import pallas as pl
from jax.experimental.pallas import tpu as pltpu
from jax.sharding import PartitionSpec as P

DK = 32
DV = 64
DOCS = 4
EPS = 1e-06
META = 8
F32 = jnp.float32
BF = jnp.bfloat16


def iota(shape, dim):
    return lax.broadcasted_iota(jnp.int32, shape, dim)

def mm(a, b, dims=((1,), (0,))):
    return lax.dot_general(a, b, (dims, ((), ())), preferred_element_type=F32)

def partner(total, upper, h):
    n = total.shape[0]
    return jnp.where(upper, pltpu.roll(total, h, 0), pltpu.roll(total, n - h, 0))

def levels(g, r):
    n = g.shape[0]
    row = iota(g.shape, 0)
    zero = jnp.zeros_like(g)
    gi, gx, ri, rx, gt, rt = g, zero, r, zero, g, r
    h = 1
    while h < n:
        upper = (row & h) != 0
        yield h, jnp.where(upper, gi, ri), jnp.where(upper, rx, gx)
        gp, rp = partner(gt, upper, h), partner(rt, upper, h)
        gi = jnp.where(upper, gi + gp, gi)
        gx = jnp.where(upper, gx, gx + gp)
        ri = jnp.where(upper, ri, ri + rp)
        rx = jnp.where(upper, rx + rp, rx)
        gt, rt = gt + gp, rt + rp
        h *= 2
    yield n, (gi, gx, gt), (ri, rx, rt)

def rows_of(docs_row):
    n = docs_row.shape[1]
    return jnp.broadcast_to(docs_row, (128, n)).T

def head_block(kw, vw):
    return (iota((kw, vw), 0) // DK) == (iota((kw, vw), 1) // DV)

def state_of(keys, values):
    kw, vw = keys.shape[1], values.shape[1]
    full = mm(keys.astype(BF), values, ((0,), (0,)))
    full = jnp.where(head_block(kw, vw), full, 0.0)
    return functools.reduce(jnp.add, [full[a : a + DK] for a in range(0, kw, DK)])

def packed(state, passing, entry, leaving):
    vw = state.shape[1]
    wide = jnp.concatenate([passing] * (vw // passing.shape[1]), axis=1)
    line = iota((META, vw), 0)
    entry = jnp.concatenate([entry] * (vw // entry.shape[1]), axis=1)
    leaving = jnp.concatenate([leaving] * (vw // leaving.shape[1]), axis=1)
    meta = jnp.where(line == 0, wide, jnp.where(line == 1, entry, leaving))
    return jnp.concatenate([state, meta], axis=0).astype(BF)

def states_kernel(q_ref, k_ref, v_ref, d_ref, doc_ref, qf_ref, qb_ref, f_ref, b_ref):
    n, kw = q_ref.shape
    docs = rows_of(doc_ref[...].astype(F32))
    first, last = docs[0:1], docs[n - 1 : n]
    for h, fwd, bwd in levels(d_ref[0], d_ref[1]):
        if h == n:
            break
    gi, gx, gt = fwd
    ri, rx, rt = bwd
    q = q_ref[...].astype(F32) * DK ** (-0.5)
    k = k_ref[...].astype(F32)
    v = v_ref[...]
    qf_ref[...] = (q * jnp.exp(gi)).astype(BF)
    qb_ref[...] = (q * jnp.exp(ri)).astype(BF)
    through = jnp.where(first == last, 1.0, 0.0)
    f_ref[...] = packed(
        state_of(jnp.where(docs == last, k * jnp.exp(gx), 0.0), v),
        jnp.exp(gt[0:1]) * through, first, last)
    b_ref[...] = packed(
        state_of(jnp.where(docs == first, k * jnp.exp(rx), 0.0), v),
        jnp.exp(rt[0:1]) * through, last, first)

def spread(passing, vw):
    kw = passing.shape[1]
    place = (iota((DK, kw), 1) % DK) == iota((DK, kw), 0)
    picked = jnp.where(place, jnp.broadcast_to(passing, (DK, kw)), 0.0)
    return mm(picked.astype(BF), jnp.where(head_block(kw, vw), 1.0, 0.0).astype(BF))

def chain3(near, mid, far, kw):
    vw = near.shape[1]
    n, m, f = near.astype(F32), mid.astype(F32), far.astype(F32)
    top = lambda a: a[:DK]
    line = lambda a, j: a[DK + j : DK + j + 1]
    keep1 = jnp.where(line(n, 1) == line(m, 2), 1.0, 0.0)
    keep2 = jnp.where(line(m, 1) == line(f, 2), 1.0, 0.0)
    p1 = (line(n, 0) * keep1)[:, :kw]
    p2 = (line(m, 0) * keep2)[:, :kw]
    state = top(n) + spread(p1, vw) * (top(m) + spread(p2, vw) * top(f))
    return state, p1 * p2 * line(f, 0)[:, :kw], line(f, 1), line(n, 2)

def fold_kernel(f1, f2, f3, b1, b2, b3, f_ref, b_ref, *, kw):
    for refs, out in (((f1, f2, f3), f_ref), ((b1, b2, b3), b_ref)):
        state, passing, entry, leaving = chain3(*(x[...] for x in refs), kw)
        out[...] = packed(state, passing, entry[:, :kw], leaving[:, :kw])

def local_kernel(q_ref, k_ref, v_ref, d_ref, doc_ref, out_ref, qe_ref, ke_ref):
    n, kw = q_ref.shape
    vw = v_ref.shape[1]
    half = n // 2
    heads = kw // DK
    q = q_ref[...].astype(F32) * DK ** (-0.5)
    k = k_ref[...].astype(F32)
    hs = []
    for h, eq, ek in levels(d_ref[0], d_ref[1]):
        if h < n:
            qe_ref[len(hs)] = (q * jnp.exp(eq)).astype(BF)
            ke_ref[len(hs)] = (k * jnp.exp(ek)).astype(BF)
            hs.append(h)
    drow = doc_ref[...].astype(F32)
    dcol = rows_of(drow)
    v = v_ref[...]
    lane = iota((half, kw), 1) // DK
    olane = iota((half, vw), 1) // DV
    apart = iota((half, half), 0) ^ iota((half, half), 1)
    ones = jnp.where(head_block(kw, vw), 2.0, 0.0).astype(BF)
    same = mm((q * k).astype(BF), ones) * v.astype(F32)
    for t in range(2):
        mine = slice(t * half, (t + 1) * half)
        other = slice((1 - t) * half, (2 - t) * half)
        ok_in = (dcol[mine] == drow[:, mine]) & (apart != 0)
        ok_off = dcol[mine] == drow[:, other]
        acc = same[mine]
        for head in range(heads):
            own = lane == head
            score = None
            for l, h in enumerate(hs[:-1]):
                prod = mm(jnp.where(own, qe_ref[l, mine], 0), ke_ref[l, mine], ((1,), (1,)))
                score = prod if score is None else jnp.where(apart >= h, prod, score)
            off = mm(jnp.where(own, qe_ref[len(hs) - 1, mine], 0), ke_ref[len(hs) - 1, other], ((1,), (1,)))
            score = jnp.where(ok_in, score, 0.0).astype(BF)
            off = jnp.where(ok_off, off, 0.0).astype(BF)
            res = mm(score, v[mine]) + mm(off, v[other])
            acc = acc + jnp.where(olane == head, res, 0.0)
        out_ref[mine] = acc

def mix_kernel(local_ref, qf_ref, qb_ref, doc_ref, gate_ref, gain_ref, f1, f2, f3, b1, b2, b3, out_ref):
    n, kw = qf_ref.shape
    vw = local_ref.shape[1]
    docs = rows_of(doc_ref[...].astype(F32))
    out = local_ref[...]
    block = head_block(kw, vw)
    for q_ref, refs in ((qf_ref, (f1, f2, f3)), (qb_ref, (b1, b2, b3))):
        state, _, _, leaving = chain3(*(x[...] for x in refs), kw)
        wide = jnp.where(block, jnp.concatenate([state] * (kw // DK), axis=0), 0.0)
        reach = jnp.where(docs[:, :kw] == leaving[:, :kw], q_ref[...], 0)
        out = out + mm(reach, wide.astype(BF))
    square = out * out
    high = square.astype(BF)
    low = (square - high.astype(F32)).astype(BF)
    mean = jnp.where((iota((vw, vw), 0) // DV) == (iota((vw, vw), 1) // DV), 1.0 / DV, 0.0).astype(BF)
    power = mm(high, mean) + mm(low, mean)
    gate = gate_ref[...].astype(F32)
    out_ref[...] = (out * lax.rsqrt(power + EPS) * gain_ref[...] * (gate / (1.0 + jnp.exp(-gate)))).astype(BF)

def call(kernel, outs, args, scratch=(), flops=1 << 26):
    return pl.pallas_call(
        kernel, out_shape=outs, scratch_shapes=scratch,
        in_specs=[pl.BlockSpec(memory_space=pltpu.VMEM)] * len(args),
        out_specs=jax.tree.map(lambda _: pl.BlockSpec(memory_space=pltpu.VMEM), outs),
        cost_estimate=pl.CostEstimate(flops=flops, bytes_accessed=1 << 20, transcendentals=1 << 17),
    )(*args)

SDS = jax.ShapeDtypeStruct
def states(q,k,v,d,doc):
    n,kw=q.shape; vw=v.shape[1]
    return call(states_kernel,(SDS((n,kw),BF),)*2+(SDS((DK+META,vw),BF),)*2,(q,k,v,d,doc))
def fold(parts,kw):
    vw=parts[0].shape[1]
    return call(functools.partial(fold_kernel,kw=kw),(SDS((DK+META,vw),BF),)*2,parts)
def local(q,k,v,d,doc):
    n,kw=q.shape; vw=v.shape[1]; L=n.bit_length()-1
    return call(local_kernel,SDS((n,vw),F32),(q,k,v,d,doc),(pltpu.VMEM((L,n,kw),BF),)*2,flops=1<<29)
def mix(local,qf,qb,doc,gate,gain,parts):
    return call(mix_kernel,SDS(local.shape,BF),(local,qf,qb,doc,gate,gain,*parts))


def ring(axis, step):
    peers = lax.axis_size(axis)
    return [(i, (i + step) % peers) for i in range(peers)]


def line(axis, step):
    peers = lax.axis_size(axis)
    return [(i, i + step) for i in range(peers) if 0 <= i + step < peers]


def carried(f, b, kw, reach):
    step = 1
    while True:
        shifts = (1, 2, 3) if step == 1 else (step, 2 * step)
        near = [lax.ppermute(f, "sp", line("sp", s)) for s in shifts]
        far = [lax.ppermute(b, "sp", line("sp", -s)) for s in shifts]
        if step > 1:
            near, far = [f] + near, [b] + far
        step *= 3
        if step >= reach:
            return tuple(near + far)
        f, b = fold(tuple(near + far), kw)


def from_peers(parts, axis):
    return [lax.ppermute(parts[s], axis, ring(axis, s)) for s in range(1, len(parts))]


def part_of(x, number, peers):
    width = x.shape[1] // peers
    return lax.dynamic_slice_in_dim(x, number * width, width, 1)


def summed(mine, axis):
    return mine + sum(from_peers([mine] * lax.axis_size(axis), axis))


def normed(stream, full_width, gain, bias):
    total = summed(jnp.stack([jnp.sum(stream, axis=1), jnp.sum(stream * stream, axis=1)]), "tp")
    middle = total[0][:, None] / full_width
    spread_ = total[1][:, None] / full_width - middle * middle
    return (stream - middle) * lax.rsqrt(spread_ + EPS) * gain + bias


def inner_kernel(at_ref, x0, x1, x2, x3, gate_ref, up_ref, out_ref):
    gate, up = None, None
    for s, x in enumerate((x0, x1, x2, x3)):
        depth = x.shape[1]
        rows = pl.ds(pl.multiple_of(at_ref[s] * depth, depth), depth)
        g, u = mm(x[...], gate_ref[rows, :]), mm(x[...], up_ref[rows, :])
        gate, up = (g, u) if s == 0 else (gate + g, up + u)
    out_ref[...] = (gate / (1.0 + jnp.exp(-gate)) * up).astype(BF)


def inner_of(at, pieces, weights, hidden):
    n, depth = pieces[0].shape
    full = weights.shape[0]
    block = 256
    steps = hidden // block
    return pl.pallas_call(
        inner_kernel,
        out_shape=SDS((n, hidden), BF),
        grid_spec=pltpu.PrefetchScalarGridSpec(
            num_scalar_prefetch=1,
            grid=(steps,),
            in_specs=[pl.BlockSpec((n, depth), lambda i, at: (0, 0))] * 4
            + [pl.BlockSpec((full, block), lambda i, at: (0, i)),
               pl.BlockSpec((full, block), lambda i, at: (0, i + steps))],
            out_specs=pl.BlockSpec((n, block), lambda i, at: (0, i)),
        ),
        cost_estimate=pl.CostEstimate(flops=4 * n * full * hidden, bytes_accessed=4 * full * hidden, transcendentals=n * hidden),
    )(at, *pieces, weights, weights)


def down_kernel(at_ref, x_ref, w_ref, out_ref):
    out_ref[...] = mm(x_ref[...], w_ref[...], ((1,), (1,))).astype(BF)


def down_of(at, inner, weights, width):
    n, hidden = inner.shape
    return pl.pallas_call(
        down_kernel,
        out_shape=SDS((n, width), BF),
        grid_spec=pltpu.PrefetchScalarGridSpec(
            num_scalar_prefetch=1,
            grid=(1,),
            in_specs=[pl.BlockSpec((n, hidden), lambda i, at: (0, 0)),
                      pl.BlockSpec((width, hidden), lambda i, at: (at[0], 2))],
            out_specs=pl.BlockSpec((n, width), lambda i, at: (0, 0)),
        ),
        cost_estimate=pl.CostEstimate(flops=2 * n * hidden * width, bytes_accessed=2 * hidden * width, transcendentals=0),
    )(at, inner, weights)


def on_device(
    queries, key_rows, value_rows, out_gate, log_decay, doc_ids, head_gain, out_weight,
    residual, norm_gain, norm_bias, gate_weight, up_weight, down_weight,
):
    peers, me = lax.axis_size("tp"), lax.axis_index("tp")
    length, kw = queries.shape
    hidden = gate_weight.shape[1]
    weights = lax.all_gather(
        jnp.concatenate([gate_weight, up_weight, down_weight.T], axis=1), "sp", axis=0, tiled=True
    )
    docs = doc_ids[None]
    qf, qb, f, b = states(queries, key_rows, value_rows, log_decay, docs)
    reach = -(-length * lax.axis_size("sp") // DOCS // length) + 1
    parts = carried(f, b, kw, reach)
    near = local(queries, key_rows, value_rows, log_decay, docs)
    mixed = mix(near, qf, qb, docs, out_gate, head_gain[None], parts)
    partial = jnp.dot(mixed, out_weight, preferred_element_type=F32).astype(BF)
    mine = [part_of(partial, (me + s) % peers, peers) for s in range(peers)]
    branch = sum(x.astype(F32) for x in [mine[0]] + from_peers(mine, "tp"))
    own_width = residual.shape[1]
    full_width = own_width * peers
    own = lambda table, j: lax.dynamic_slice_in_dim(table[j], me * own_width, own_width, 0)
    settled = normed(residual.astype(F32) + branch, full_width, own(norm_gain, 0), own(norm_bias, 0))
    features = settled.astype(BF)
    pieces = [features] + from_peers([features] * peers, "tp")
    at = jnp.stack([(me - s) % peers for s in range(peers)]).astype(jnp.int32)
    inner = inner_of(at, pieces, weights, hidden)
    down = [None] * peers
    for s in [2, 1, 3, 0]:
        down[s] = down_of(((me + s) % peers).astype(jnp.int32)[None], inner, weights, own_width)
    total = sum(x.astype(F32) for x in [down[0]] + from_peers(down, "tp"))
    result = normed(settled + 0.5 * total, full_width, own(norm_gain, 1), own(norm_bias, 1))
    return result.astype(BF)


def solution(mesh):
    rows = ("grp", "sp")
    in_specs = (
        P(rows, "tp"), P(rows, "tp"), P(rows, "tp"), P(rows, "tp"), P(None, rows, "tp"),
        P(rows), P("tp"), P("tp", None), P(rows, "tp"), P(), P(),
        P("sp", "tp"), P("sp", "tp"), P("tp", "sp"),
    )
    return jax.shard_map(
        on_device, mesh=mesh, in_specs=in_specs, out_specs=P(rows, "tp"), check_vma=False
    )
```

```python
import functools
import jax
import jax.numpy as jnp
from jax import lax
from jax.experimental import pallas as pl
from jax.experimental.pallas import tpu as pltpu
from jax.sharding import PartitionSpec as P

DK = 32
DV = 64
DOCS = 4
EPS = 1e-06
META = 8
F32 = jnp.float32
BF = jnp.bfloat16


def iota(shape, dim):
    return lax.broadcasted_iota(jnp.int32, shape, dim)

def mm(a, b, dims=((1,), (0,))):
    return lax.dot_general(a, b, (dims, ((), ())), preferred_element_type=F32)

def partner(total, upper, h):
    n = total.shape[0]
    return jnp.where(upper, pltpu.roll(total, h, 0), pltpu.roll(total, n - h, 0))

def levels(g, r):
    n = g.shape[0]
    row = iota(g.shape, 0)
    zero = jnp.zeros_like(g)
    gi, gx, ri, rx, gt, rt = g, zero, r, zero, g, r
    h = 1
    while h < n:
        upper = (row & h) != 0
        yield h, jnp.where(upper, gi, ri), jnp.where(upper, rx, gx)
        gp, rp = partner(gt, upper, h), partner(rt, upper, h)
        gi = jnp.where(upper, gi + gp, gi)
        gx = jnp.where(upper, gx, gx + gp)
        ri = jnp.where(upper, ri, ri + rp)
        rx = jnp.where(upper, rx + rp, rx)
        gt, rt = gt + gp, rt + rp
        h *= 2
    yield n, (gi, gx, gt), (ri, rx, rt)

def rows_of(docs_row):
    n = docs_row.shape[1]
    return jnp.broadcast_to(docs_row, (128, n)).T

def head_block(kw, vw):
    return (iota((kw, vw), 0) // DK) == (iota((kw, vw), 1) // DV)

def state_of(keys, values):
    kw, vw = keys.shape[1], values.shape[1]
    full = mm(keys.astype(BF), values, ((0,), (0,)))
    full = jnp.where(head_block(kw, vw), full, 0.0)
    return functools.reduce(jnp.add, [full[a : a + DK] for a in range(0, kw, DK)])

def packed(state, passing, entry, leaving):
    vw = state.shape[1]
    wide = jnp.concatenate([passing] * (vw // passing.shape[1]), axis=1)
    line = iota((META, vw), 0)
    entry = jnp.concatenate([entry] * (vw // entry.shape[1]), axis=1)
    leaving = jnp.concatenate([leaving] * (vw // leaving.shape[1]), axis=1)
    meta = jnp.where(line == 0, wide, jnp.where(line == 1, entry, leaving))
    return jnp.concatenate([state, meta], axis=0).astype(BF)

def states_kernel(q_ref, k_ref, v_ref, d_ref, doc_ref, qf_ref, qb_ref, f_ref, b_ref):
    n, kw = q_ref.shape
    docs = rows_of(doc_ref[...].astype(F32))
    first, last = docs[0:1], docs[n - 1 : n]
    for h, fwd, bwd in levels(d_ref[0], d_ref[1]):
        if h == n:
            break
    gi, gx, gt = fwd
    ri, rx, rt = bwd
    q = q_ref[...].astype(F32) * DK ** (-0.5)
    k = k_ref[...].astype(F32)
    v = v_ref[...]
    qf_ref[...] = (q * jnp.exp(gi)).astype(BF)
    qb_ref[...] = (q * jnp.exp(ri)).astype(BF)
    through = jnp.where(first == last, 1.0, 0.0)
    f_ref[...] = packed(
        state_of(jnp.where(docs == last, k * jnp.exp(gx), 0.0), v),
        jnp.exp(gt[0:1]) * through, first, last)
    b_ref[...] = packed(
        state_of(jnp.where(docs == first, k * jnp.exp(rx), 0.0), v),
        jnp.exp(rt[0:1]) * through, last, first)

def spread(passing, vw):
    kw = passing.shape[1]
    place = (iota((DK, kw), 1) % DK) == iota((DK, kw), 0)
    picked = jnp.where(place, jnp.broadcast_to(passing, (DK, kw)), 0.0)
    return mm(picked.astype(BF), jnp.where(head_block(kw, vw), 1.0, 0.0).astype(BF))

def chain3(near, mid, far, kw):
    vw = near.shape[1]
    n, m, f = near.astype(F32), mid.astype(F32), far.astype(F32)
    top = lambda a: a[:DK]
    line = lambda a, j: a[DK + j : DK + j + 1]
    keep1 = jnp.where(line(n, 1) == line(m, 2), 1.0, 0.0)
    keep2 = jnp.where(line(m, 1) == line(f, 2), 1.0, 0.0)
    p1 = (line(n, 0) * keep1)[:, :kw]
    p2 = (line(m, 0) * keep2)[:, :kw]
    state = top(n) + spread(p1, vw) * (top(m) + spread(p2, vw) * top(f))
    return state, p1 * p2 * line(f, 0)[:, :kw], line(f, 1), line(n, 2)

def fold_kernel(f1, f2, f3, b1, b2, b3, f_ref, b_ref, *, kw):
    for refs, out in (((f1, f2, f3), f_ref), ((b1, b2, b3), b_ref)):
        state, passing, entry, leaving = chain3(*(x[...] for x in refs), kw)
        out[...] = packed(state, passing, entry[:, :kw], leaving[:, :kw])

def local_kernel(q_ref, k_ref, v_ref, d_ref, doc_ref, out_ref, qe_ref, ke_ref):
    n, kw = q_ref.shape
    vw = v_ref.shape[1]
    half = n // 2
    heads = kw // DK
    q = q_ref[...].astype(F32) * DK ** (-0.5)
    k = k_ref[...].astype(F32)
    hs = []
    for h, eq, ek in levels(d_ref[0], d_ref[1]):
        if h < n:
            qe_ref[len(hs)] = (q * jnp.exp(eq)).astype(BF)
            ke_ref[len(hs)] = (k * jnp.exp(ek)).astype(BF)
            hs.append(h)
    drow = doc_ref[...].astype(F32)
    dcol = rows_of(drow)
    v = v_ref[...]
    lane = iota((half, kw), 1) // DK
    olane = iota((half, vw), 1) // DV
    apart = iota((half, half), 0) ^ iota((half, half), 1)
    ones = jnp.where(head_block(kw, vw), 2.0, 0.0).astype(BF)
    same = mm((q * k).astype(BF), ones) * v.astype(F32)
    for t in range(2):
        mine = slice(t * half, (t + 1) * half)
        other = slice((1 - t) * half, (2 - t) * half)
        ok_in = (dcol[mine] == drow[:, mine]) & (apart != 0)
        ok_off = dcol[mine] == drow[:, other]
        acc = same[mine]
        for head in range(heads):
            own = lane == head
            score = None
            for l, h in enumerate(hs[:-1]):
                prod = mm(jnp.where(own, qe_ref[l, mine], 0), ke_ref[l, mine], ((1,), (1,)))
                score = prod if score is None else jnp.where(apart >= h, prod, score)
            off = mm(jnp.where(own, qe_ref[len(hs) - 1, mine], 0), ke_ref[len(hs) - 1, other], ((1,), (1,)))
            score = jnp.where(ok_in, score, 0.0).astype(BF)
            off = jnp.where(ok_off, off, 0.0).astype(BF)
            res = mm(score, v[mine]) + mm(off, v[other])
            acc = acc + jnp.where(olane == head, res, 0.0)
        out_ref[mine] = acc

def mix_kernel(to_ref, local_ref, qf_ref, qb_ref, doc_ref, gate_ref, gain_ref, f1, f2, f3, b1, b2, b3, *outs):
    n, kw = qf_ref.shape
    vw = local_ref.shape[1]
    docs = rows_of(doc_ref[...].astype(F32))
    out = local_ref[...]
    block = head_block(kw, vw)
    for q_ref, refs in ((qf_ref, (f1, f2, f3)), (qb_ref, (b1, b2, b3))):
        state, _, _, leaving = chain3(*(x[...] for x in refs), kw)
        wide = jnp.where(block, jnp.concatenate([state] * (kw // DK), axis=0), 0.0)
        reach = jnp.where(docs[:, :kw] == leaving[:, :kw], q_ref[...], 0)
        out = out + mm(reach, wide.astype(BF))
    square = out * out
    high = square.astype(BF)
    low = (square - high.astype(F32)).astype(BF)
    mean = jnp.where((iota((vw, vw), 0) // DV) == (iota((vw, vw), 1) // DV), 1.0 / DV, 0.0).astype(BF)
    power = mm(high, mean) + mm(low, mean)
    gate = gate_ref[...].astype(F32)
    all_ref = outs[-1]
    all_ref[...] = (out * lax.rsqrt(power + EPS) * gain_ref[...] * (gate / (1.0 + jnp.exp(-gate)))).astype(BF)
    for s, part in enumerate(outs[:-1]):
        rows = part.shape[0]
        part[...] = all_ref[pl.ds(pl.multiple_of(to_ref[s] * rows, rows), rows)]

SDS = jax.ShapeDtypeStruct
VMEM = pl.BlockSpec(memory_space=pltpu.VMEM)
SMEM = pl.BlockSpec(memory_space=pltpu.SMEM)
ANY = pl.BlockSpec(memory_space=pl.ANY)


def call(kernel, outs, args, scratch=(), flops=1 << 26, specs=None, mib=8):
    return pl.pallas_call(
        kernel, out_shape=outs, scratch_shapes=scratch,
        in_specs=specs or [VMEM] * len(args),
        out_specs=jax.tree.map(lambda _: VMEM, outs),
        cost_estimate=pl.CostEstimate(flops=flops, bytes_accessed=1 << 20, transcendentals=1 << 17),
        compiler_params=pltpu.CompilerParams(vmem_limit_bytes=mib << 20),
    )(*args)


def states(q, k, v, d, doc):
    n, kw = q.shape
    vw = v.shape[1]
    outs = (SDS((n, kw), BF),) * 2 + (SDS((DK + META, vw), BF),) * 2
    return call(states_kernel, outs, (q, k, v, d, doc))


def fold(parts, kw):
    vw = parts[0].shape[1]
    return call(functools.partial(fold_kernel, kw=kw), (SDS((DK + META, vw), BF),) * 2, parts)


def local(q, k, v, d, doc):
    n, kw = q.shape
    vw = v.shape[1]
    scratch = (pltpu.VMEM((n.bit_length() - 1, n, kw), BF),) * 2
    return call(local_kernel, SDS((n, vw), F32), (q, k, v, d, doc), scratch, flops=1 << 29)


def mix(to, near, qf, qb, doc, gate, gain, parts, peers):
    n, vw = near.shape
    args = (to, near, qf, qb, doc, gate, gain, *parts)
    return call(mix_kernel, (SDS((n // peers, vw), BF),) * peers, args, (pltpu.VMEM((n, vw), BF),),
                specs=[SMEM] + [VMEM] * (len(args) - 1))


def layer_norm(stream, gain, bias):
    width = stream.shape[1]
    middle = jnp.sum(stream, axis=1, keepdims=True) / width
    offset = stream - middle
    spread = jnp.sum(offset * offset, axis=1, keepdims=True) / width
    return offset * lax.rsqrt(spread + EPS) * gain + bias


def settle_kernel(from_ref, *refs, peers):
    mixed, weights, residual = (refs[j * peers : (j + 1) * peers] for j in range(3))
    gain_ref, bias_ref, settled_ref, features_ref, stream_ref = refs[3 * peers :]
    for s in range(peers):
        width = residual[s].shape[1]
        cols = pl.ds(pl.multiple_of(from_ref[s] * width, width), width)
        stream_ref[:, cols] = residual[s][...].astype(F32)
    stream = stream_ref[...]
    for s in range(peers):
        stream = stream + mm(mixed[s][...], weights[s][...]).astype(BF).astype(F32)
    settled = layer_norm(stream, gain_ref[0:1], bias_ref[0:1])
    settled_ref[...] = settled
    features_ref[...] = settled.astype(BF)


def settle(came, mixed, weights, residual, gain, bias):
    peers = len(mixed)
    rows, width = mixed[0].shape[0], weights[0].shape[1]
    args = (came, *mixed, *weights, *residual, gain, bias)
    return call(functools.partial(settle_kernel, peers=peers), (SDS((rows, width), F32), SDS((rows, width), BF)),
                args, (pltpu.VMEM((rows, width), F32),), flops=1 << 28, mib=12,
                specs=[SMEM] + [VMEM] * (len(args) - 1))


def forward_kernel(*refs, peers, hidden, cuts, outs):
    pieces, w, down = refs[:peers], refs[peers], refs[peers + 1 : 2 * peers + 1]
    x_ref, w_ref, inner_ref, sem = refs[2 * peers + 1 :]
    n, full = pieces[0].shape
    b, ob = hidden // cuts, full // outs

    def taken(rows, cols, j):
        return pltpu.make_async_copy(w.at[rows, cols], w_ref.at[rows, cols], sem.at[j])

    copies = [taken(slice(None), slice(part * hidden + j * b, part * hidden + (j + 1) * b), 2 * j + part)
              for j in range(cuts) for part in range(2)]
    copies += [taken(slice(o * ob, (o + 1) * ob), slice(2 * hidden, 3 * hidden), 2 * cuts + o) for o in range(outs)]
    for copy in copies:
        copy.start()
    for s in range(peers):
        x_ref[s * n : (s + 1) * n] = pieces[s][...]
    for j in range(cuts):
        copies[2 * j].wait()
        gate = mm(x_ref[...], w_ref[:, j * b : (j + 1) * b])
        copies[2 * j + 1].wait()
        up = mm(x_ref[...], w_ref[:, hidden + j * b : hidden + (j + 1) * b])
        inner_ref[:, j * b : (j + 1) * b] = (gate / (1.0 + jnp.exp(-gate)) * up).astype(BF)
    for o in range(outs):
        copies[2 * cuts + o].wait()
        rows = slice(o * ob, (o + 1) * ob)
        total = mm(inner_ref[...], w_ref[rows, 2 * hidden :], ((1,), (1,))).astype(BF)
        for s in range(peers):
            down[-s % peers][:, rows] = total[s * n : (s + 1) * n]


def forward(pieces, weights, hidden, cuts=2, outs=2):
    peers = len(pieces)
    n, full = pieces[0].shape
    return call(
        functools.partial(forward_kernel, peers=peers, hidden=hidden, cuts=cuts, outs=outs),
        (SDS((n, full), BF),) * peers, (*pieces, weights),
        (pltpu.VMEM((peers * n, full), BF), pltpu.VMEM(weights.shape, BF), pltpu.VMEM((peers * n, hidden), BF),
         pltpu.SemaphoreType.DMA((2 * cuts + outs,))),
        flops=6 * peers * n * full * hidden, specs=[VMEM] * peers + [ANY], mib=56)


def finish_kernel(to_ref, settled_ref, *refs, peers):
    down = refs[:peers]
    gain_ref, bias_ref = refs[peers : peers + 2]
    outs, all_ref = refs[peers + 2 : -1], refs[-1]
    total = down[0][...].astype(F32)
    for s in range(1, peers):
        total = total + down[s][...].astype(F32)
    all_ref[...] = layer_norm(settled_ref[...] + 0.5 * total, gain_ref[1:2], bias_ref[1:2])
    for s in range(peers):
        width = outs[s].shape[1]
        outs[s][...] = all_ref[:, pl.ds(pl.multiple_of(to_ref[s] * width, width), width)].astype(BF)


def finish(to, settled, down, gain, bias):
    peers = len(down)
    n, full = settled.shape
    args = (to, settled, *down, gain, bias)
    return call(functools.partial(finish_kernel, peers=peers), (SDS((n, full // peers), BF),) * peers, args,
                (pltpu.VMEM((n, full), F32),), specs=[SMEM] + [VMEM] * (len(args) - 1))


def placed_kernel(from_ref, *refs):
    for s, part in enumerate(refs[:-1]):
        rows = part.shape[0]
        refs[-1][pl.ds(pl.multiple_of(from_ref[s] * rows, rows), rows)] = part[...]


def placed(came, parts):
    n, width = parts[0].shape
    return call(placed_kernel, SDS((len(parts) * n, width), BF), (came, *parts),
                specs=[SMEM] + [VMEM] * len(parts))


def ring(axis, step):
    peers = lax.axis_size(axis)
    return [(i, (i + step) % peers) for i in range(peers)]


def line(axis, step):
    peers = lax.axis_size(axis)
    return [(i, i + step) for i in range(peers) if 0 <= i + step < peers]


def carried(f, b, kw, reach):
    step = 1
    while True:
        shifts = (1, 2, 3) if step == 1 else (step, 2 * step)
        near = [lax.ppermute(f, "sp", line("sp", s)) for s in shifts]
        far = [lax.ppermute(b, "sp", line("sp", -s)) for s in shifts]
        if step > 1:
            near, far = [f] + near, [b] + far
        step *= 3
        if step >= reach:
            return tuple(near + far)
        f, b = fold(tuple(near + far), kw)


def from_peers(parts, axis):
    return [lax.ppermute(parts[s], axis, ring(axis, s)) for s in range(1, len(parts))]


def swapped(parts, axis):
    return [parts[0]] + from_peers(parts, axis)


def on_device(
    queries, key_rows, value_rows, out_gate, log_decay, doc_ids, head_gain, out_weight,
    residual, norm_gain, norm_bias, gate_weight, up_weight, down_weight,
):
    peers, me = lax.axis_size("tp"), lax.axis_index("tp")
    length, kw = queries.shape
    hidden = gate_weight.shape[1]
    own = length // peers
    to = jnp.stack([(me + s) % peers for s in range(peers)]).astype(jnp.int32)
    came = jnp.stack([(me - s) % peers for s in range(peers)]).astype(jnp.int32)
    weights = lax.all_gather(
        jnp.concatenate([gate_weight, up_weight, down_weight.T], axis=1), "sp", axis=0, tiled=True
    )
    out_weights = swapped([out_weight] * peers, "tp")
    streams = swapped(
        [lax.dynamic_slice_in_dim(residual, to[s] * own, own, 0) for s in range(peers)], "tp"
    )
    docs = doc_ids[None]
    qf, qb, f, b = states(queries, key_rows, value_rows, log_decay, docs)
    reach = -(-length * lax.axis_size("sp") // DOCS // length) + 1
    parts = carried(f, b, kw, reach)
    near = local(queries, key_rows, value_rows, log_decay, docs)
    mixed = swapped(mix(to, near, qf, qb, docs, out_gate, head_gain[None], parts, peers), "tp")
    settled, features = settle(came, mixed, out_weights, streams, norm_gain, norm_bias)
    pieces = swapped([features] * peers, "tp")
    down = swapped(forward(pieces, weights, hidden), "tp")
    return placed(came, swapped(finish(to, settled, down, norm_gain, norm_bias), "tp"))


def solution(mesh):
    rows = ("grp", "sp")
    in_specs = (
        P(rows, "tp"), P(rows, "tp"), P(rows, "tp"), P(rows, "tp"), P(None, rows, "tp"),
        P(rows), P("tp"), P("tp", None), P(rows, "tp"), P(), P(),
        P("sp", "tp"), P("sp", "tp"), P("tp", "sp"),
    )
    return jax.shard_map(
        on_device, mesh=mesh, in_specs=in_specs, out_specs=P(rows, "tp"), check_vma=False
    )
```

```python
import functools
import jax
import jax.numpy as jnp
from jax import lax
from jax.experimental import pallas as pl
from jax.experimental.pallas import tpu as pltpu
from jax.sharding import PartitionSpec as P

DK = 32
DV = 64
DOCS = 4
EPS = 1e-06
META = 8
F32 = jnp.float32
BF = jnp.bfloat16


def iota(shape, dim):
    return lax.broadcasted_iota(jnp.int32, shape, dim)

def mm(a, b, dims=((1,), (0,))):
    return lax.dot_general(a, b, (dims, ((), ())), preferred_element_type=F32)

def partner(total, upper, h):
    n = total.shape[0]
    return jnp.where(upper, pltpu.roll(total, h, 0), pltpu.roll(total, n - h, 0))

def levels(g, r):
    n = g.shape[0]
    row = iota(g.shape, 0)
    zero = jnp.zeros_like(g)
    gi, gx, ri, rx, gt, rt = g, zero, r, zero, g, r
    h = 1
    while h < n:
        upper = (row & h) != 0
        yield h, jnp.where(upper, gi, ri), jnp.where(upper, rx, gx)
        gp, rp = partner(gt, upper, h), partner(rt, upper, h)
        gi = jnp.where(upper, gi + gp, gi)
        gx = jnp.where(upper, gx, gx + gp)
        ri = jnp.where(upper, ri, ri + rp)
        rx = jnp.where(upper, rx + rp, rx)
        gt, rt = gt + gp, rt + rp
        h *= 2
    yield n, (gi, gx, gt), (ri, rx, rt)

def rows_of(docs_row):
    n = docs_row.shape[1]
    return jnp.broadcast_to(docs_row, (128, n)).T

def head_block(kw, vw):
    return (iota((kw, vw), 0) // DK) == (iota((kw, vw), 1) // DV)

def state_of(keys, values):
    kw, vw = keys.shape[1], values.shape[1]
    full = mm(keys.astype(BF), values, ((0,), (0,)))
    full = jnp.where(head_block(kw, vw), full, 0.0)
    return functools.reduce(jnp.add, [full[a : a + DK] for a in range(0, kw, DK)])

def packed(state, passing, entry, leaving):
    vw = state.shape[1]
    wide = jnp.concatenate([passing] * (vw // passing.shape[1]), axis=1)
    line = iota((META, vw), 0)
    entry = jnp.concatenate([entry] * (vw // entry.shape[1]), axis=1)
    leaving = jnp.concatenate([leaving] * (vw // leaving.shape[1]), axis=1)
    meta = jnp.where(line == 0, wide, jnp.where(line == 1, entry, leaving))
    return jnp.concatenate([state, meta], axis=0).astype(BF)

def states_kernel(q_ref, k_ref, v_ref, d_ref, doc_ref, qf_ref, qb_ref, f_ref, b_ref, docs_ref):
    n, kw = q_ref.shape
    docs = rows_of(doc_ref[...].astype(F32))
    docs_ref[...] = docs
    first, last = docs[0:1], docs[n - 1 : n]
    for h, fwd, bwd in levels(d_ref[0], d_ref[1]):
        if h == n:
            break
    gi, gx, gt = fwd
    ri, rx, rt = bwd
    q = q_ref[...].astype(F32) * DK ** (-0.5)
    k = k_ref[...].astype(F32)
    v = v_ref[...]
    qf_ref[...] = (q * jnp.exp(gi)).astype(BF)
    qb_ref[...] = (q * jnp.exp(ri)).astype(BF)
    through = jnp.where(first == last, 1.0, 0.0)
    f_ref[...] = packed(
        state_of(jnp.where(docs == last, k * jnp.exp(gx), 0.0), v),
        jnp.exp(gt[0:1]) * through, first, last)
    b_ref[...] = packed(
        state_of(jnp.where(docs == first, k * jnp.exp(rx), 0.0), v),
        jnp.exp(rt[0:1]) * through, last, first)

def spread(passing, vw):
    kw = passing.shape[1]
    place = (iota((DK, kw), 1) % DK) == iota((DK, kw), 0)
    picked = jnp.where(place, jnp.broadcast_to(passing, (DK, kw)), 0.0)
    return mm(picked.astype(BF), jnp.where(head_block(kw, vw), 1.0, 0.0).astype(BF))

def chain3(near, mid, far, kw):
    vw = near.shape[1]
    n, m, f = near.astype(F32), mid.astype(F32), far.astype(F32)
    top = lambda a: a[:DK]
    line = lambda a, j: a[DK + j : DK + j + 1]
    keep1 = jnp.where(line(n, 1) == line(m, 2), 1.0, 0.0)
    keep2 = jnp.where(line(m, 1) == line(f, 2), 1.0, 0.0)
    p1 = (line(n, 0) * keep1)[:, :kw]
    p2 = (line(m, 0) * keep2)[:, :kw]
    state = top(n) + spread(p1, vw) * (top(m) + spread(p2, vw) * top(f))
    return state, p1 * p2 * line(f, 0)[:, :kw], line(f, 1), line(n, 2)

def fold_kernel(f1, f2, f3, b1, b2, b3, f_ref, b_ref, *, kw):
    for refs, out in (((f1, f2, f3), f_ref), ((b1, b2, b3), b_ref)):
        state, passing, entry, leaving = chain3(*(x[...] for x in refs), kw)
        out[...] = packed(state, passing, entry[:, :kw], leaving[:, :kw])

def local_kernel(q_ref, k_ref, v_ref, d_ref, doc_ref, gate_ref, gain_ref, out_ref, factor_ref, qe_ref, ke_ref):
    n, kw = q_ref.shape
    vw = v_ref.shape[1]
    half = n // 2
    gate = gate_ref[...].astype(F32)
    factor_ref[...] = gain_ref[...] * (gate / (1.0 + jnp.exp(-gate)))
    heads = kw // DK
    q = q_ref[...].astype(F32) * DK ** (-0.5)
    k = k_ref[...].astype(F32)
    hs = []
    for h, eq, ek in levels(d_ref[0], d_ref[1]):
        if h < n:
            qe_ref[len(hs)] = (q * jnp.exp(eq)).astype(BF)
            ke_ref[len(hs)] = (k * jnp.exp(ek)).astype(BF)
            hs.append(h)
    drow = doc_ref[...].astype(F32)
    dcol = rows_of(drow)
    v = v_ref[...]
    lane = iota((half, kw), 1) // DK
    olane = iota((half, vw), 1) // DV
    apart = iota((half, half), 0) ^ iota((half, half), 1)
    ones = jnp.where(head_block(kw, vw), 2.0, 0.0).astype(BF)
    same = mm((q * k).astype(BF), ones) * v.astype(F32)
    for t in range(2):
        mine = slice(t * half, (t + 1) * half)
        other = slice((1 - t) * half, (2 - t) * half)
        ok_in = (dcol[mine] == drow[:, mine]) & (apart != 0)
        ok_off = dcol[mine] == drow[:, other]
        acc = same[mine]
        for head in range(heads):
            own = lane == head
            score = None
            for l, h in enumerate(hs[:-1]):
                prod = mm(jnp.where(own, qe_ref[l, mine], 0), ke_ref[l, mine], ((1,), (1,)))
                score = prod if score is None else jnp.where(apart >= h, prod, score)
            off = mm(jnp.where(own, qe_ref[len(hs) - 1, mine], 0), ke_ref[len(hs) - 1, other], ((1,), (1,)))
            score = jnp.where(ok_in, score, 0.0).astype(BF)
            off = jnp.where(ok_off, off, 0.0).astype(BF)
            res = mm(score, v[mine]) + mm(off, v[other])
            acc = acc + jnp.where(olane == head, res, 0.0)
        out_ref[mine] = acc

def mix_kernel(near_ref, factor_ref, qf_ref, qb_ref, docs_ref, f1, f2, f3, b1, b2, b3, *outs):
    n, kw = qf_ref.shape
    vw = near_ref.shape[1]
    docs = docs_ref[...]
    out = near_ref[...]
    block = head_block(kw, vw)
    for q_ref, refs in ((qf_ref, (f1, f2, f3)), (qb_ref, (b1, b2, b3))):
        state, _, _, leaving = chain3(*(x[...] for x in refs), kw)
        wide = jnp.where(block, jnp.concatenate([state] * (kw // DK), axis=0), 0.0)
        reach = jnp.where(docs[:, :kw] == leaving[:, :kw], q_ref[...], 0)
        out = out + mm(reach, wide.astype(BF))
    square = out * out
    high = square.astype(BF)
    low = (square - high.astype(F32)).astype(BF)
    mean = jnp.where((iota((vw, vw), 0) // DV) == (iota((vw, vw), 1) // DV), 1.0 / DV, 0.0).astype(BF)
    power = mm(high, mean) + mm(low, mean)
    all_ref = outs[-1]
    all_ref[...] = (out * lax.rsqrt(power + EPS) * factor_ref[...]).astype(BF)
    for s, part in enumerate(outs[:-1]):
        part[...] = all_ref[place(s, part.shape[0])]


SDS = jax.ShapeDtypeStruct
VMEM = pl.BlockSpec(memory_space=pltpu.VMEM)


def call(kernel, outs, args, scratch=(), flops=1 << 26, mib=8):
    return pl.pallas_call(
        kernel, out_shape=outs, scratch_shapes=scratch,
        in_specs=[VMEM] * len(args),
        out_specs=jax.tree.map(lambda _: VMEM, outs),
        cost_estimate=pl.CostEstimate(flops=flops, bytes_accessed=1 << 20, transcendentals=1 << 17),
        compiler_params=pltpu.CompilerParams(vmem_limit_bytes=mib << 20),
    )(*args)


def states(q, k, v, d, doc):
    n, kw = q.shape
    vw = v.shape[1]
    outs = (SDS((n, kw), BF),) * 2 + (SDS((DK + META, vw), BF),) * 2
    return call(states_kernel, outs + (SDS((n, 128), F32),), (q, k, v, d, doc), mib=62)


def fold(parts, kw):
    vw = parts[0].shape[1]
    return call(functools.partial(fold_kernel, kw=kw), (SDS((DK + META, vw), BF),) * 2, parts)


def local(q, k, v, d, doc, gate, gain):
    n, kw = q.shape
    vw = v.shape[1]
    scratch = (pltpu.VMEM((n.bit_length() - 1, n, kw), BF),) * 2
    return call(local_kernel, (SDS((n, vw), F32),) * 2, (q, k, v, d, doc, gate, gain), scratch, flops=1 << 29, mib=62)


def mix(near, factor, qf, qb, docs, parts, peers):
    n, vw = near.shape
    return call(mix_kernel, (SDS((n // peers, vw), BF),) * peers, (near, factor, qf, qb, docs, *parts),
                scratch=(pltpu.VMEM((n, vw), BF),), mib=62)


def place(step, width):
    peers = lax.axis_size("tp")
    number = lax.rem(lax.axis_index("tp") + step + peers, peers)
    return pl.ds(pl.multiple_of(number * width, width), width)


def layer_norm(stream, gain, bias):
    width = stream.shape[1]
    middle = jnp.sum(stream, axis=1, keepdims=True) / width
    offset = stream - middle
    spread = jnp.sum(offset * offset, axis=1, keepdims=True) / width
    return offset * lax.rsqrt(spread + EPS) * gain + bias


def settle_kernel(*refs, peers):
    mixed, weights, residual = (refs[j * peers : (j + 1) * peers] for j in range(3))
    gain_ref, bias_ref, settled_ref, features_ref, stream_ref = refs[3 * peers :]
    for s in range(peers):
        width = residual[s].shape[1]
        stream_ref[:, place(-s, width)] = residual[s][...].astype(F32)
    stream = stream_ref[...]
    for s in range(peers):
        stream = stream + mm(mixed[s][...], weights[s][...]).astype(BF).astype(F32)
    settled = layer_norm(stream, gain_ref[0:1], bias_ref[0:1])
    settled_ref[...] = settled
    features_ref[...] = settled.astype(BF)


def settle(mixed, weights, residual, gain, bias):
    peers = len(mixed)
    rows, width = mixed[0].shape[0], weights[0].shape[1]
    args = (*mixed, *weights, *residual, gain, bias)
    return call(functools.partial(settle_kernel, peers=peers), (SDS((rows, width), F32), SDS((rows, width), BF)),
                args, (pltpu.VMEM((rows, width), F32),), flops=1 << 28, mib=12)


def forward_kernel(*refs, count, hidden, cut):
    pieces, w_ref, down, inner_ref = refs[:count], refs[count], refs[count + 1 : 2 * count + 1], refs[-1]
    x = jnp.concatenate([piece[...] for piece in pieces], axis=0) if count > 1 else pieces[0][...]
    n, full = pieces[0].shape
    for j in range(0, hidden, cut):
        gate = mm(x, w_ref[:, j : j + cut])
        up = mm(x, w_ref[:, hidden + j : hidden + j + cut])
        inner_ref[:, j : j + cut] = (gate / (1.0 + jnp.exp(-gate)) * up).astype(BF)
    total = mm(inner_ref[...], w_ref[:, 2 * hidden :], ((1,), (1,))).astype(BF)
    for s in range(count):
        down[s][...] = total[s * n : (s + 1) * n]


def forward(pieces, weights, hidden, cut=384):
    count = len(pieces)
    n, full = pieces[0].shape
    return call(
        functools.partial(forward_kernel, count=count, hidden=hidden, cut=cut),
        (SDS((n, full), BF),) * count, (*pieces, weights), scratch=(pltpu.VMEM((count * n, hidden), BF),),
        flops=6 * count * n * full * hidden, mib=8)


def finish_kernel(settled_ref, *refs, peers):
    down = refs[:peers]
    gain_ref, bias_ref = refs[peers : peers + 2]
    outs, all_ref = refs[peers + 2 : -1], refs[-1]
    total = down[0][...].astype(F32)
    for s in range(1, peers):
        total = total + down[s][...].astype(F32)
    all_ref[...] = layer_norm(settled_ref[...] + 0.5 * total, gain_ref[1:2], bias_ref[1:2])
    for s in range(peers):
        outs[s][...] = all_ref[:, place(s, outs[s].shape[1])].astype(BF)


def finish(settled, down, gain, bias):
    peers = len(down)
    n, full = settled.shape
    return call(functools.partial(finish_kernel, peers=peers), (SDS((n, full // peers), BF),) * peers,
                (settled, *down, gain, bias), (pltpu.VMEM((n, full), F32),))


def placed_kernel(*refs):
    for s, part in enumerate(refs[:-1]):
        refs[-1][place(-s, part.shape[0])] = part[...]


def placed(parts):
    n, width = parts[0].shape
    return call(placed_kernel, SDS((len(parts) * n, width), BF), parts)


def ring(axis, step):
    peers = lax.axis_size(axis)
    return [(i, (i + step) % peers) for i in range(peers)]


def line(axis, step):
    peers = lax.axis_size(axis)
    return [(i, i + step) for i in range(peers) if 0 <= i + step < peers]


def carried(f, b, kw, reach):
    step = 1
    while True:
        shifts = (1, 2, 3) if step == 1 else (step, 2 * step)
        near = [lax.ppermute(f, "sp", line("sp", s)) for s in shifts]
        far = [lax.ppermute(b, "sp", line("sp", -s)) for s in shifts]
        if step > 1:
            near, far = [f] + near, [b] + far
        step *= 3
        if step >= reach:
            return tuple(near + far)
        f, b = fold(tuple(near + far), kw)


def from_peers(parts, axis):
    return [lax.ppermute(parts[s], axis, ring(axis, s)) for s in range(1, len(parts))]


def swapped(parts, axis):
    return [parts[0]] + from_peers(parts, axis)


def on_device(
    queries, key_rows, value_rows, out_gate, log_decay, doc_ids, head_gain, out_weight,
    residual, norm_gain, norm_bias, gate_weight, up_weight, down_weight,
):
    peers, me = lax.axis_size("tp"), lax.axis_index("tp")
    length, kw = queries.shape
    hidden = gate_weight.shape[1]
    own = length // peers
    weights = lax.all_gather(
        jnp.concatenate([gate_weight, up_weight, down_weight.T], axis=1), "sp", axis=0, tiled=True
    )
    docs = doc_ids[None]
    qf, qb, f, b, where = states(queries, key_rows, value_rows, log_decay, docs)
    reach = -(-length * lax.axis_size("sp") // DOCS // length) + 1
    parts = carried(f, b, kw, reach)
    out_weight, _ = lax.optimization_barrier((out_weight, f))
    out_weights = swapped([out_weight] * peers, "tp")
    near, factor = local(queries, key_rows, value_rows, log_decay, docs, out_gate, head_gain[None])
    residual, _ = lax.optimization_barrier((residual, near))
    streams = swapped(
        [lax.dynamic_slice_in_dim(residual, (me + s) % peers * own, own, 0) for s in range(peers)], "tp"
    )
    mixed = swapped(mix(near, factor, qf, qb, where, parts, peers), "tp")
    settled, features = settle(mixed, out_weights, streams, norm_gain, norm_bias)
    pieces = swapped([features] * peers, "tp")
    down = [None] * peers
    for group in ([2], [1, 3], [0]):
        for s, part in zip(group, forward([pieces[-s % peers] for s in group], weights, hidden)):
            down[s] = part
    return placed(swapped(finish(settled, swapped(down, "tp"), norm_gain, norm_bias), "tp"))


def solution(mesh):
    rows = ("grp", "sp")
    in_specs = (
        P(rows, "tp"), P(rows, "tp"), P(rows, "tp"), P(rows, "tp"), P(None, rows, "tp"),
        P(rows), P("tp"), P("tp", None), P(rows, "tp"), P(), P(),
        P("sp", "tp"), P("sp", "tp"), P("tp", "sp"),
    )
    return jax.shard_map(
        on_device, mesh=mesh, in_specs=in_specs, out_specs=P(rows, "tp"), check_vma=False
    )
```

```python
import functools
import jax
import jax.numpy as jnp
from jax import lax
from jax.experimental import pallas as pl
from jax.experimental.pallas import tpu as pltpu
from jax.sharding import PartitionSpec as P

DK = 32
DV = 64
DOCS = 4
EPS = 1e-06
META = 8
STREAM_MIB = 40
F32 = jnp.float32
BF = jnp.bfloat16


def iota(shape, dim):
    return lax.broadcasted_iota(jnp.int32, shape, dim)

def mm(a, b, dims=((1,), (0,))):
    return lax.dot_general(a, b, (dims, ((), ())), preferred_element_type=F32)

def partner(total, upper, h):
    n = total.shape[0]
    return jnp.where(upper, pltpu.roll(total, h, 0), pltpu.roll(total, n - h, 0))

def levels(g, r):
    n = g.shape[0]
    row = iota(g.shape, 0)
    zero = jnp.zeros_like(g)
    gi, gx, ri, rx, gt, rt = g, zero, r, zero, g, r
    h = 1
    while h < n:
        upper = (row & h) != 0
        yield h, jnp.where(upper, gi, ri), jnp.where(upper, rx, gx)
        gp, rp = partner(gt, upper, h), partner(rt, upper, h)
        gi = jnp.where(upper, gi + gp, gi)
        gx = jnp.where(upper, gx, gx + gp)
        ri = jnp.where(upper, ri, ri + rp)
        rx = jnp.where(upper, rx + rp, rx)
        gt, rt = gt + gp, rt + rp
        h *= 2
    yield n, (gi, gx, gt), (ri, rx, rt)

def rows_of(docs_row):
    n = docs_row.shape[1]
    return jnp.broadcast_to(docs_row, (128, n)).T

def head_block(kw, vw):
    return (iota((kw, vw), 0) // DK) == (iota((kw, vw), 1) // DV)

def state_of(keys, values):
    kw, vw = keys.shape[1], values.shape[1]
    full = mm(keys.astype(BF), values, ((0,), (0,)))
    full = jnp.where(head_block(kw, vw), full, 0.0)
    return functools.reduce(jnp.add, [full[a : a + DK] for a in range(0, kw, DK)])

def packed(state, passing, entry, leaving):
    vw = state.shape[1]
    wide = jnp.concatenate([passing] * (vw // passing.shape[1]), axis=1)
    line = iota((META, vw), 0)
    entry = jnp.concatenate([entry] * (vw // entry.shape[1]), axis=1)
    leaving = jnp.concatenate([leaving] * (vw // leaving.shape[1]), axis=1)
    meta = jnp.where(line == 0, wide, jnp.where(line == 1, entry, leaving))
    return jnp.concatenate([state, meta], axis=0)

def states_kernel(q_ref, k_ref, v_ref, d_ref, doc_ref, qf_ref, qb_ref, keep_ref, give_ref, docs_ref):
    n, kw = q_ref.shape
    docs = rows_of(doc_ref[...].astype(F32))
    docs_ref[...] = docs
    first, last = docs[0:1], docs[n - 1 : n]
    for h, fwd, bwd in levels(d_ref[0], d_ref[1]):
        if h == n:
            break
    gi, gx, gt = fwd
    ri, rx, rt = bwd
    q = q_ref[...].astype(F32) * DK ** (-0.5)
    k = k_ref[...].astype(F32)
    v = v_ref[...]
    qf_ref[...] = (q * jnp.exp(gi)).astype(BF)
    qb_ref[...] = (q * jnp.exp(ri)).astype(BF)
    through = jnp.where(first == last, 1.0, 0.0)
    ahead = packed(
        state_of(jnp.where(docs == last, k * jnp.exp(gx), 0.0), v),
        jnp.exp(gt[0:1]) * through, first, last)
    back = packed(
        state_of(jnp.where(docs == first, k * jnp.exp(rx), 0.0), v),
        jnp.exp(rt[0:1]) * through, last, first)
    low = on_low_core()
    keep_ref[...] = jnp.where(low, ahead, back).astype(BF)
    give_ref[...] = jnp.where(low, back, ahead).astype(BF)


def on_low_core():
    return lax.rem(lax.axis_index("sp"), 2) == 0


def spread(passing, vw):
    kw = passing.shape[1]
    place = (iota((DK, kw), 1) % DK) == iota((DK, kw), 0)
    picked = jnp.where(place, jnp.broadcast_to(passing, (DK, kw)), 0.0)
    return mm(picked.astype(BF), jnp.where(head_block(kw, vw), 1.0, 0.0).astype(BF))

def chained(links, kw):
    line = lambda a, j: a[DK + j : DK + j + 1]
    vw = links[0].shape[1]
    state, passing = links[-1][:DK], line(links[-1], 0)[:, :kw]
    for near, far in reversed(list(zip(links[:-1], links[1:]))):
        through = (line(near, 0) * jnp.where(line(near, 1) == line(far, 2), 1.0, 0.0))[:, :kw]
        state = near[:DK] + spread(through, vw) * state
        passing = passing * through
    return packed(state, passing, line(links[-1], 1)[:, :kw], line(links[0], 2)[:, :kw])


def pair_kernel(keep_ref, came_ref, out_ref, *, kw):
    out_ref[...] = chained([came_ref[...].astype(F32), keep_ref[...].astype(F32)], kw).astype(BF)


def entering_kernel(keep_ref, *refs, kw):
    out_ref, give_ref = refs[-2:]
    incoming = chained([ref[...].astype(F32) for ref in refs[:-2]], kw)
    out_ref[...] = incoming.astype(BF)
    give_ref[...] = chained([keep_ref[...].astype(F32), incoming], kw).astype(BF)


def local_kernel(q_ref, k_ref, v_ref, d_ref, doc_ref, gate_ref, gain_ref, out_ref, factor_ref, qe_ref, ke_ref):
    n, kw = q_ref.shape
    vw = v_ref.shape[1]
    half = n // 2
    gate = gate_ref[...].astype(F32)
    factor_ref[...] = gain_ref[...] * (gate / (1.0 + jnp.exp(-gate)))
    heads = kw // DK
    q = q_ref[...].astype(F32) * DK ** (-0.5)
    k = k_ref[...].astype(F32)
    hs = []
    for h, eq, ek in levels(d_ref[0], d_ref[1]):
        if h < n:
            qe_ref[len(hs)] = (q * jnp.exp(eq)).astype(BF)
            ke_ref[len(hs)] = (k * jnp.exp(ek)).astype(BF)
            hs.append(h)
    drow = doc_ref[...].astype(F32)
    dcol = rows_of(drow)
    v = v_ref[...]
    lane = iota((half, kw), 1) // DK
    olane = iota((half, vw), 1) // DV
    apart = iota((half, half), 0) ^ iota((half, half), 1)
    ones = jnp.where(head_block(kw, vw), 2.0, 0.0).astype(BF)
    same = mm((q * k).astype(BF), ones) * v.astype(F32)
    for t in range(2):
        mine = slice(t * half, (t + 1) * half)
        other = slice((1 - t) * half, (2 - t) * half)
        ok_in = (dcol[mine] == drow[:, mine]) & (apart != 0)
        ok_off = dcol[mine] == drow[:, other]
        acc = same[mine]
        for head in range(heads):
            own = lane == head
            score = None
            for l, h in enumerate(hs[:-1]):
                prod = mm(jnp.where(own, qe_ref[l, mine], 0), ke_ref[l, mine], ((1,), (1,)))
                score = prod if score is None else jnp.where(apart >= h, prod, score)
            off = mm(jnp.where(own, qe_ref[len(hs) - 1, mine], 0), ke_ref[len(hs) - 1, other], ((1,), (1,)))
            score = jnp.where(ok_in, score, 0.0).astype(BF)
            off = jnp.where(ok_off, off, 0.0).astype(BF)
            res = mm(score, v[mine]) + mm(off, v[other])
            acc = acc + jnp.where(olane == head, res, 0.0)
        out_ref[mine] = acc

def mix_kernel(near_ref, factor_ref, qf_ref, qb_ref, docs_ref, mine_ref, other_ref, *outs):
    n, kw = qf_ref.shape
    vw = near_ref.shape[1]
    docs = docs_ref[...]
    out = near_ref[...]
    block = head_block(kw, vw)
    mine, other, low = mine_ref[...].astype(F32), other_ref[...].astype(F32), on_low_core()
    for q_ref, link in ((qf_ref, jnp.where(low, mine, other)), (qb_ref, jnp.where(low, other, mine))):
        state, leaving = link[:DK], link[DK + 2 : DK + 3]
        wide = jnp.where(block, jnp.concatenate([state] * (kw // DK), axis=0), 0.0)
        reach = jnp.where(docs[:, :kw] == leaving[:, :kw], q_ref[...], 0)
        out = out + mm(reach, wide.astype(BF))
    square = out * out
    high = square.astype(BF)
    low = (square - high.astype(F32)).astype(BF)
    mean = jnp.where((iota((vw, vw), 0) // DV) == (iota((vw, vw), 1) // DV), 1.0 / DV, 0.0).astype(BF)
    power = mm(high, mean) + mm(low, mean)
    all_ref = outs[-1]
    all_ref[...] = (out * lax.rsqrt(power + EPS) * factor_ref[...]).astype(BF)
    for s, part in enumerate(outs[:-1]):
        part[...] = all_ref[place(s, part.shape[0])]


SDS = jax.ShapeDtypeStruct
VMEM = pl.BlockSpec(memory_space=pltpu.VMEM)
ANY = pl.BlockSpec(memory_space=pl.ANY)


def call(kernel, outs, args, scratch=(), flops=1 << 26, mib=8, far=False):
    return pl.pallas_call(
        kernel, out_shape=outs, scratch_shapes=scratch,
        in_specs=[VMEM] * (len(args) - far) + [ANY] * far,
        out_specs=jax.tree.map(lambda _: VMEM, outs),
        cost_estimate=pl.CostEstimate(flops=flops, bytes_accessed=1 << 20, transcendentals=1 << 17),
        compiler_params=pltpu.CompilerParams(vmem_limit_bytes=mib << 20),
    )(*args)


def states(q, k, v, d, doc):
    n, kw = q.shape
    vw = v.shape[1]
    outs = (SDS((n, kw), BF),) * 2 + (SDS((DK + META, vw), BF),) * 2
    return call(states_kernel, outs + (SDS((n, 128), F32),), (q, k, v, d, doc), mib=62)


def pair(keep, came, kw):
    return call(functools.partial(pair_kernel, kw=kw), SDS(keep.shape, BF), (keep, came))


def entering(keep, links, kw):
    return call(functools.partial(entering_kernel, kw=kw), (SDS(keep.shape, BF),) * 2, (keep, *links))


def local(q, k, v, d, doc, gate, gain):
    n, kw = q.shape
    vw = v.shape[1]
    scratch = (pltpu.VMEM((n.bit_length() - 1, n, kw), BF),) * 2
    return call(local_kernel, (SDS((n, vw), F32),) * 2, (q, k, v, d, doc, gate, gain), scratch, flops=1 << 29, mib=62)


def mix(near, factor, qf, qb, docs, parts, peers):
    n, vw = near.shape
    return call(mix_kernel, (SDS((n // peers, vw), BF),) * peers, (near, factor, qf, qb, docs, *parts),
                scratch=(pltpu.VMEM((n, vw), BF),), mib=62)


def place(step, width):
    peers = lax.axis_size("tp")
    number = lax.rem(lax.axis_index("tp") + step + peers, peers)
    return pl.ds(pl.multiple_of(number * width, width), width)


def layer_norm(stream, gain, bias):
    width = stream.shape[1]
    middle = jnp.sum(stream, axis=1, keepdims=True) / width
    offset = stream - middle
    spread = jnp.sum(offset * offset, axis=1, keepdims=True) / width
    return offset * lax.rsqrt(spread + EPS) * gain + bias


def settle_kernel(*refs, peers):
    mixed, weights, residual = (refs[j * peers : (j + 1) * peers] for j in range(3))
    gain_ref, bias_ref, settled_ref, features_ref, stream_ref = refs[3 * peers :]
    for s in range(peers):
        width = residual[s].shape[1]
        stream_ref[:, place(-s, width)] = residual[s][...].astype(F32)
    stream = stream_ref[...]
    for s in range(peers):
        stream = stream + mm(mixed[s][...], weights[s][...]).astype(BF).astype(F32)
    settled = layer_norm(stream, gain_ref[0:1], bias_ref[0:1])
    settled_ref[...] = settled
    features_ref[...] = settled.astype(BF)


def settle(mixed, weights, residual, gain, bias):
    peers = len(mixed)
    rows, width = mixed[0].shape[0], weights[0].shape[1]
    args = (*mixed, *weights, *residual, gain, bias)
    return call(functools.partial(settle_kernel, peers=peers), (SDS((rows, width), F32), SDS((rows, width), BF)),
                args, (pltpu.VMEM((rows, width), F32),), flops=1 << 28, mib=12)


def forward_kernel(*refs, count, hidden, cut, streams):
    pieces, w_ref, down, inner_ref = refs[:count], refs[count], refs[count + 1 : 2 * count + 1], refs[-1]
    n, full = pieces[0].shape
    steps = hidden // cut
    if streams:
        source, w_ref, inner_ref, sem = w_ref, *refs[-3:]
        starts = [part * hidden + j * cut for j in range(steps) for part in range(2)] + [2 * hidden]
        ends = [start + cut for start in starts[:-1]] + [3 * hidden]
        copies = [pltpu.make_async_copy(source.at[:, a:b], w_ref.at[:, a:b], sem.at[k])
                  for k, (a, b) in enumerate(zip(starts, ends))]
        for copy in copies:
            copy.start()
    ready = lambda k: copies[k].wait() if streams else None
    x = jnp.concatenate([piece[...] for piece in pieces], axis=0) if count > 1 else pieces[0][...]
    for j in range(steps):
        a, b = j * cut, (j + 1) * cut
        ready(2 * j)
        gate = mm(x, w_ref[:, a:b])
        ready(2 * j + 1)
        up = mm(x, w_ref[:, hidden + a : hidden + b])
        inner_ref[:, a:b] = (gate / (1.0 + jnp.exp(-gate)) * up).astype(BF)
    ready(2 * steps)
    total = mm(inner_ref[...], w_ref[:, 2 * hidden :], ((1,), (1,))).astype(BF)
    for s in range(count):
        down[s][...] = total[s * n : (s + 1) * n]


def forward(pieces, weights, hidden, streams=False, cut=384):
    count = len(pieces)
    n, full = pieces[0].shape
    outs = (SDS((n, full), BF),) * count
    scratch = (pltpu.VMEM((count * n, hidden), BF),)
    if streams:
        outs += (SDS(weights.shape, BF),)
        scratch += (pltpu.SemaphoreType.DMA((2 * hidden // cut + 1,)),)
    return call(
        functools.partial(forward_kernel, count=count, hidden=hidden, cut=cut, streams=streams),
        outs, (*pieces, weights), scratch, flops=6 * count * n * full * hidden,
        mib=STREAM_MIB if streams else 8, far=streams)


def finish_kernel(settled_ref, *refs, peers):
    down = refs[:peers]
    gain_ref, bias_ref = refs[peers : peers + 2]
    outs, all_ref = refs[peers + 2 : -1], refs[-1]
    total = down[0][...].astype(F32)
    for s in range(1, peers):
        total = total + down[s][...].astype(F32)
    all_ref[...] = layer_norm(settled_ref[...] + 0.5 * total, gain_ref[1:2], bias_ref[1:2])
    for s in range(peers):
        outs[s][...] = all_ref[:, place(s, outs[s].shape[1])].astype(BF)


def finish(settled, down, gain, bias):
    peers = len(down)
    n, full = settled.shape
    return call(functools.partial(finish_kernel, peers=peers), (SDS((n, full // peers), BF),) * peers,
                (settled, *down, gain, bias), (pltpu.VMEM((n, full), F32),))


def placed_kernel(*refs):
    for s, part in enumerate(refs[:-1]):
        refs[-1][place(-s, part.shape[0])] = part[...]


def placed(parts):
    n, width = parts[0].shape
    return call(placed_kernel, SDS((len(parts) * n, width), BF), parts)


def ring(axis, step):
    peers = lax.axis_size(axis)
    return [(i, (i + step) % peers) for i in range(peers)]


def across(step):
    peers = lax.axis_size("sp")
    moves = [(i, i + 2 * step if i % 2 == 0 else i - 2 * step) for i in range(peers)]
    return [(i, j) for i, j in moves if 0 <= j < peers]


def other_core(x):
    return lax.ppermute(x, "sp", [(i, i ^ 1) for i in range(lax.axis_size("sp"))])


def carried(keep, give, kw, reach):
    whole = pair(keep, other_core(give), kw)
    links = [lax.ppermute(whole, "sp", across(step)) for step in range(1, -(-reach // 2) + 1)]
    mine, give = entering(keep, links, kw)
    return mine, other_core(give)


def from_peers(parts, axis):
    return [lax.ppermute(parts[s], axis, ring(axis, s)) for s in range(1, len(parts))]


def swapped(parts, axis):
    return [parts[0]] + from_peers(parts, axis)


def on_device(
    queries, key_rows, value_rows, out_gate, log_decay, doc_ids, head_gain, out_weight,
    residual, norm_gain, norm_bias, gate_weight, up_weight, down_weight,
):
    peers, me = lax.axis_size("tp"), lax.axis_index("tp")
    length, kw = queries.shape
    hidden = gate_weight.shape[1]
    own = length // peers
    weights = lax.all_gather(
        jnp.concatenate([gate_weight, up_weight, down_weight.T], axis=1), "sp", axis=0, tiled=True
    )
    docs = doc_ids[None]
    qf, qb, keep, give, where = states(queries, key_rows, value_rows, log_decay, docs)
    reach = -(-length * lax.axis_size("sp") // DOCS // length) + 1
    parts = carried(keep, give, kw, reach)
    out_weight, _ = lax.optimization_barrier((out_weight, give))
    out_weights = swapped([out_weight] * peers, "tp")
    near, factor = local(queries, key_rows, value_rows, log_decay, docs, out_gate, head_gain[None])
    residual, _ = lax.optimization_barrier((residual, near))
    streams = swapped(
        [lax.dynamic_slice_in_dim(residual, (me + s) % peers * own, own, 0) for s in range(peers)], "tp"
    )
    mixed = swapped(mix(near, factor, qf, qb, where, parts, peers), "tp")
    settled, features = settle(mixed, out_weights, streams, norm_gain, norm_bias)
    pieces = swapped([features] * peers, "tp")
    down = [None] * peers
    for group in ([1, 3], [2], [0]):
        *parts, = forward([pieces[-s % peers] for s in group], weights, hidden, streams=group == [1, 3])
        if group == [1, 3]:
            weights = parts.pop()
        for s, part in zip(group, parts):
            down[s] = part
    return placed(swapped(finish(settled, swapped(down, "tp"), norm_gain, norm_bias), "tp"))


def solution(mesh):
    rows = ("grp", "sp")
    in_specs = (
        P(rows, "tp"), P(rows, "tp"), P(rows, "tp"), P(rows, "tp"), P(None, rows, "tp"),
        P(rows), P("tp"), P("tp", None), P(rows, "tp"), P(), P(),
        P("sp", "tp"), P("sp", "tp"), P("tp", "sp"),
    )
    return jax.shard_map(
        on_device, mesh=mesh, in_specs=in_specs, out_specs=P(rows, "tp"), check_vma=False
    )
```

```python
import functools
import jax
import jax.numpy as jnp
from jax import lax
from jax.experimental import pallas as pl
from jax.experimental.pallas import tpu as pltpu
from jax.sharding import PartitionSpec as P


DK = 32
DV = 64
DOCS = 4
EPS = 1e-06
META = 8
STREAM_MIB = 40
F32 = jnp.float32
BF = jnp.bfloat16


def iota(shape, dim):
    return lax.broadcasted_iota(jnp.int32, shape, dim)


def mm(a, b, dims=((1,), (0,))):
    return lax.dot_general(a, b, (dims, ((), ())), preferred_element_type=F32)


def partner(total, upper, h):
    n = total.shape[0]
    return jnp.where(upper, pltpu.roll(total, h, 0), pltpu.roll(total, n - h, 0))


def levels(g, r):
    n = g.shape[0]
    row = iota(g.shape, 0)
    zero = jnp.zeros_like(g)
    gi, gx, ri, rx, gt, rt = g, zero, r, zero, g, r
    h = 1
    while h < n:
        upper = (row & h) != 0
        yield h, jnp.where(upper, gi, ri), jnp.where(upper, rx, gx)
        gp, rp = partner(gt, upper, h), partner(rt, upper, h)
        gi = jnp.where(upper, gi + gp, gi)
        gx = jnp.where(upper, gx, gx + gp)
        ri = jnp.where(upper, ri, ri + rp)
        rx = jnp.where(upper, rx + rp, rx)
        gt, rt = gt + gp, rt + rp
        h *= 2
    yield n, (gi, gx, gt), (ri, rx, rt)


def rows_of(docs_row):
    n = docs_row.shape[1]
    return jnp.broadcast_to(docs_row, (128, n)).T


def head_block(kw, vw):
    return (iota((kw, vw), 0) // DK) == (iota((kw, vw), 1) // DV)


def state_of(keys, values):
    kw, vw = keys.shape[1], values.shape[1]
    full = mm(keys.astype(BF), values, ((0,), (0,)))
    full = jnp.where(head_block(kw, vw), full, 0.0)
    return functools.reduce(jnp.add, [full[a : a + DK] for a in range(0, kw, DK)])


def packed(state, passing, entry, leaving):
    vw = state.shape[1]
    wide = jnp.concatenate([passing] * (vw // passing.shape[1]), axis=1)
    line = iota((META, vw), 0)
    entry = jnp.concatenate([entry] * (vw // entry.shape[1]), axis=1)
    leaving = jnp.concatenate([leaving] * (vw // leaving.shape[1]), axis=1)
    meta = jnp.where(line == 0, wide, jnp.where(line == 1, entry, leaving))
    return jnp.concatenate([state, meta], axis=0)


def states_kernel(q_ref, k_ref, v_ref, d_ref, doc_ref, qf_ref, qb_ref, keep_ref, give_ref, docs_ref):
    n, _ = q_ref.shape
    docs = rows_of(doc_ref[...].astype(F32))
    docs_ref[...] = docs
    first, last = docs[0:1], docs[n - 1 : n]
    for h, fwd, bwd in levels(d_ref[0], d_ref[1]):
        if h == n:
            break
    gi, gx, gt = fwd
    ri, rx, rt = bwd
    q = q_ref[...].astype(F32) * DK ** (-0.5)
    k = k_ref[...].astype(F32)
    v = v_ref[...]
    qf_ref[...] = (q * jnp.exp(gi)).astype(BF)
    qb_ref[...] = (q * jnp.exp(ri)).astype(BF)
    through = jnp.where(first == last, 1.0, 0.0)
    ahead = packed(
        state_of(jnp.where(docs == last, k * jnp.exp(gx), 0.0), v),
        jnp.exp(gt[0:1]) * through, first, last)
    back = packed(
        state_of(jnp.where(docs == first, k * jnp.exp(rx), 0.0), v),
        jnp.exp(rt[0:1]) * through, last, first)
    low = on_low_core()
    keep_ref[...] = jnp.where(low, ahead, back).astype(BF)
    give_ref[...] = jnp.where(low, back, ahead).astype(BF)


def on_low_core():
    return lax.rem(lax.axis_index("sp"), 2) == 0


def spread(passing, vw):
    kw = passing.shape[1]
    place = (iota((DK, kw), 1) % DK) == iota((DK, kw), 0)
    picked = jnp.where(place, jnp.broadcast_to(passing, (DK, kw)), 0.0)
    return mm(picked.astype(BF), jnp.where(head_block(kw, vw), 1.0, 0.0).astype(BF))


def chained(links, kw):
    line = lambda a, j: a[DK + j : DK + j + 1]
    vw = links[0].shape[1]
    state, passing = links[-1][:DK], line(links[-1], 0)[:, :kw]
    for near, far in reversed(list(zip(links[:-1], links[1:]))):
        through = (line(near, 0) * jnp.where(line(near, 1) == line(far, 2), 1.0, 0.0))[:, :kw]
        state = near[:DK] + spread(through, vw) * state
        passing = passing * through
    return packed(state, passing, line(links[-1], 1)[:, :kw], line(links[0], 2)[:, :kw])


def pair_kernel(keep_ref, came_ref, out_ref, *, kw):
    out_ref[...] = chained([came_ref[...].astype(F32), keep_ref[...].astype(F32)], kw).astype(BF)


def entering_kernel(keep_ref, *refs, kw):
    out_ref, give_ref = refs[-2:]
    incoming = chained([ref[...].astype(F32) for ref in refs[:-2]], kw)
    out_ref[...] = incoming.astype(BF)
    give_ref[...] = chained([keep_ref[...].astype(F32), incoming], kw).astype(BF)


def local_kernel(q_ref, k_ref, v_ref, d_ref, doc_ref, gate_ref, gain_ref, out_ref, factor_ref, qe_ref, ke_ref):
    n, kw = q_ref.shape
    vw = v_ref.shape[1]
    half = n // 2
    gate = gate_ref[...].astype(F32)
    factor_ref[...] = gain_ref[...] * (gate / (1.0 + jnp.exp(-gate)))
    heads = kw // DK
    q = q_ref[...].astype(F32) * DK ** (-0.5)
    k = k_ref[...].astype(F32)
    hs = []
    for h, eq, ek in levels(d_ref[0], d_ref[1]):
        if h < n:
            qe_ref[len(hs)] = (q * jnp.exp(eq)).astype(BF)
            ke_ref[len(hs)] = (k * jnp.exp(ek)).astype(BF)
            hs.append(h)
    drow = doc_ref[...].astype(F32)
    dcol = rows_of(drow)
    v = v_ref[...]
    lane = iota((half, kw), 1) // DK
    olane = iota((half, vw), 1) // DV
    apart = iota((half, half), 0) ^ iota((half, half), 1)
    ones = jnp.where(head_block(kw, vw), 2.0, 0.0).astype(BF)
    same = mm((q * k).astype(BF), ones) * v.astype(F32)
    for t in range(2):
        mine = slice(t * half, (t + 1) * half)
        other = slice((1 - t) * half, (2 - t) * half)
        ok_in = (dcol[mine] == drow[:, mine]) & (apart != 0)
        ok_off = dcol[mine] == drow[:, other]
        acc = same[mine]
        for head in range(heads):
            own = lane == head
            score = None
            for l, h in enumerate(hs[:-1]):
                prod = mm(jnp.where(own, qe_ref[l, mine], 0), ke_ref[l, mine], ((1,), (1,)))
                score = prod if score is None else jnp.where(apart >= h, prod, score)
            off = mm(jnp.where(own, qe_ref[len(hs) - 1, mine], 0), ke_ref[len(hs) - 1, other], ((1,), (1,)))
            score = jnp.where(ok_in, score, 0.0).astype(BF)
            off = jnp.where(ok_off, off, 0.0).astype(BF)
            res = mm(score, v[mine]) + mm(off, v[other])
            acc = acc + jnp.where(olane == head, res, 0.0)
        out_ref[mine] = acc


def mix_kernel(near_ref, factor_ref, qf_ref, qb_ref, docs_ref, mine_ref, other_ref, *outs):
    _, kw = qf_ref.shape
    vw = near_ref.shape[1]
    docs = docs_ref[...]
    out = near_ref[...]
    block = head_block(kw, vw)
    mine, other, low = mine_ref[...].astype(F32), other_ref[...].astype(F32), on_low_core()
    for q_ref, link in ((qf_ref, jnp.where(low, mine, other)), (qb_ref, jnp.where(low, other, mine))):
        state, leaving = link[:DK], link[DK + 2 : DK + 3]
        wide = jnp.where(block, jnp.concatenate([state] * (kw // DK), axis=0), 0.0)
        reach = jnp.where(docs[:, :kw] == leaving[:, :kw], q_ref[...], 0)
        out = out + mm(reach, wide.astype(BF))
    square = out * out
    high = square.astype(BF)
    low = (square - high.astype(F32)).astype(BF)
    mean = jnp.where((iota((vw, vw), 0) // DV) == (iota((vw, vw), 1) // DV), 1.0 / DV, 0.0).astype(BF)
    power = mm(high, mean) + mm(low, mean)
    all_ref = outs[-1]
    all_ref[...] = (out * lax.rsqrt(power + EPS) * factor_ref[...]).astype(BF)
    for s, part in enumerate(outs[:-1]):
        part[...] = all_ref[place(s, part.shape[0])]


SDS = jax.ShapeDtypeStruct
VMEM = pl.BlockSpec(memory_space=pltpu.VMEM)
ANY = pl.BlockSpec(memory_space=pl.ANY)


def call(kernel, outs, args, scratch=(), flops=1 << 26, mib=8, far=False):
    return pl.pallas_call(
        kernel, out_shape=outs, scratch_shapes=scratch,
        in_specs=[VMEM] * (len(args) - far) + [ANY] * far,
        out_specs=jax.tree.map(lambda _: VMEM, outs),
        cost_estimate=pl.CostEstimate(flops=flops, bytes_accessed=1 << 20, transcendentals=1 << 17),
        compiler_params=pltpu.CompilerParams(vmem_limit_bytes=mib << 20),
    )(*args)


def states(q, k, v, d, doc):
    n, kw = q.shape
    vw = v.shape[1]
    outs = (SDS((n, kw), BF),) * 2 + (SDS((DK + META, vw), BF),) * 2
    return call(states_kernel, outs + (SDS((n, 128), F32),), (q, k, v, d, doc), mib=62)


def pair(keep, came, kw):
    return call(functools.partial(pair_kernel, kw=kw), SDS(keep.shape, BF), (keep, came))


def entering(keep, links, kw):
    return call(functools.partial(entering_kernel, kw=kw), (SDS(keep.shape, BF),) * 2, (keep, *links))


def local(q, k, v, d, doc, gate, gain):
    n, kw = q.shape
    vw = v.shape[1]
    scratch = (pltpu.VMEM((n.bit_length() - 1, n, kw), BF),) * 2
    return call(local_kernel, (SDS((n, vw), F32),) * 2, (q, k, v, d, doc, gate, gain), scratch, flops=1 << 29, mib=62)


def mix(near, factor, qf, qb, docs, parts, peers):
    n, vw = near.shape
    return call(mix_kernel, (SDS((n // peers, vw), BF),) * peers, (near, factor, qf, qb, docs, *parts),
                scratch=(pltpu.VMEM((n, vw), BF),), mib=62)


def place(step, width):
    peers = lax.axis_size("tp")
    number = lax.rem(lax.axis_index("tp") + step + peers, peers)
    return pl.ds(pl.multiple_of(number * width, width), width)


def layer_norm(stream, gain, bias):
    width = stream.shape[1]
    middle = jnp.sum(stream, axis=1, keepdims=True) / width
    offset = stream - middle
    spread = jnp.sum(offset * offset, axis=1, keepdims=True) / width
    return offset * lax.rsqrt(spread + EPS) * gain + bias


def settle_kernel(*refs, peers):
    mixed, weights, residual = (refs[j * peers : (j + 1) * peers] for j in range(3))
    gain_ref, bias_ref, settled_ref, features_ref, stream_ref = refs[3 * peers :]
    for s in range(peers):
        width = residual[s].shape[1]
        stream_ref[:, place(-s, width)] = residual[s][...].astype(F32)
    stream = stream_ref[...]
    for s in range(peers):
        stream = stream + mm(mixed[s][...], weights[s][...]).astype(BF).astype(F32)
    settled = layer_norm(stream, gain_ref[0:1], bias_ref[0:1])
    settled_ref[...] = settled
    features_ref[...] = settled.astype(BF)


def settle(mixed, weights, residual, gain, bias):
    peers = len(mixed)
    rows, width = mixed[0].shape[0], weights[0].shape[1]
    args = (*mixed, *weights, *residual, gain, bias)
    return call(functools.partial(settle_kernel, peers=peers), (SDS((rows, width), F32), SDS((rows, width), BF)),
                args, (pltpu.VMEM((rows, width), F32),), flops=1 << 28, mib=12)


def forward_kernel(*refs, count, hidden, cut, streams, sizes):
    pieces, w_ref, down, inner_ref = refs[:count], refs[count], refs[count + 1 : count + 1 + len(sizes)], refs[-1]
    _, full = pieces[0].shape
    steps = hidden // cut
    if streams:
        source, w_ref, inner_ref, sem = w_ref, *refs[-3:]
        spans = [(slice(0, full), slice(part * hidden + j * cut, part * hidden + (j + 1) * cut))
                 for j in range(steps) for part in range(2)]
        spans += [(slice(o, o + full // 2), slice(2 * hidden, 3 * hidden)) for o in range(0, full, full // 2)]
        copies = [pltpu.make_async_copy(source.at[span], w_ref.at[span], sem.at[k]) for k, span in enumerate(spans)]
        for copy in copies:
            copy.start()
    ready = lambda k: copies[k].wait() if streams else None
    x = jnp.concatenate([piece[...] for piece in pieces], axis=0) if count > 1 else pieces[0][...]
    for j in range(steps):
        a, b = j * cut, (j + 1) * cut
        ready(2 * j)
        gate = mm(x, w_ref[:, a:b])
        ready(2 * j + 1)
        up = mm(x, w_ref[:, hidden + a : hidden + b])
        inner_ref[:, a:b] = (gate / (1.0 + jnp.exp(-gate)) * up).astype(BF)
    for o in range(2):
        rows = slice(o * full // 2, (o + 1) * full // 2)
        ready(2 * steps + o)
        total = mm(inner_ref[...], w_ref[rows, 2 * hidden :], ((1,), (1,))).astype(BF)
        for s, size in enumerate(sizes):
            down[s][:, rows] = total[sum(sizes[:s]) : sum(sizes[: s + 1])]


def forward(pieces, weights, hidden, streams=False, cut=384, sizes=None):
    count = len(pieces)
    n, full = pieces[0].shape
    sizes = sizes or (n,) * count
    outs = tuple(SDS((size, full), BF) for size in sizes)
    scratch = (pltpu.VMEM((count * n, hidden), BF),)
    if streams:
        outs += (SDS(weights.shape, BF),)
        scratch += (pltpu.SemaphoreType.DMA((2 * hidden // cut + 2,)),)
    return call(
        functools.partial(forward_kernel, count=count, hidden=hidden, cut=cut, streams=streams, sizes=sizes),
        outs, (*pieces, weights), scratch, flops=6 * count * n * full * hidden,
        mib=STREAM_MIB if streams else 8, far=streams)


def finish_kernel(settled_ref, *refs, peers, count):
    down = refs[:count]
    gain_ref, bias_ref = refs[count : count + 2]
    outs, all_ref = refs[count + 2 : -1], refs[-1]
    total = down[0][...].astype(F32)
    for part in down[1 : peers - 1]:
        total = total + part[...].astype(F32)
    total = total + jnp.concatenate([part[...].astype(F32) for part in down[peers - 1 :]], axis=0)
    all_ref[...] = layer_norm(settled_ref[...] + 0.5 * total, gain_ref[1:2], bias_ref[1:2])
    for s in range(peers):
        outs[s][...] = all_ref[:, place(s, outs[s].shape[1])].astype(BF)


def finish(settled, down, gain, bias, peers):
    n, full = settled.shape
    return call(functools.partial(finish_kernel, peers=peers, count=len(down)), (SDS((n, full // peers), BF),) * peers,
                (settled, *down, gain, bias), (pltpu.VMEM((n, full), F32),))


def placed_kernel(*refs):
    for s, part in enumerate(refs[:-1]):
        refs[-1][place(-s, part.shape[0])] = part[...]


def placed(parts):
    n, width = parts[0].shape
    return call(placed_kernel, SDS((len(parts) * n, width), BF), parts)


def ring(axis, step):
    peers = lax.axis_size(axis)
    return [(i, (i + step) % peers) for i in range(peers)]


def across(step):
    peers = lax.axis_size("sp")
    moves = [(i, i + 2 * step if i % 2 == 0 else i - 2 * step) for i in range(peers)]
    return [(i, j) for i, j in moves if 0 <= j < peers]


def other_core(x):
    return lax.ppermute(x, "sp", [(i, i ^ 1) for i in range(lax.axis_size("sp"))])


def carried(keep, give, kw, reach):
    whole = pair(keep, other_core(give), kw)
    links = [lax.ppermute(whole, "sp", across(step)) for step in range(1, -(-reach // 2) + 1)]
    mine, give = entering(keep, links, kw)
    return mine, other_core(give)


def from_peers(parts, axis):
    return [lax.ppermute(parts[s], axis, ring(axis, s)) for s in range(1, len(parts))]


def swapped(parts, axis):
    return [parts[0]] + from_peers(parts, axis)


def on_device(
    queries, key_rows, value_rows, out_gate, log_decay, doc_ids, head_gain, out_weight,
    residual, norm_gain, norm_bias, gate_weight, up_weight, down_weight,
):
    peers, me = lax.axis_size("tp"), lax.axis_index("tp")
    length, kw = queries.shape
    hidden = gate_weight.shape[1]
    own = length // peers
    weights = lax.all_gather(
        jnp.concatenate([gate_weight, up_weight, down_weight.T], axis=1), "sp", axis=0, tiled=True
    )
    docs = doc_ids[None]
    qf, qb, keep, give, where = states(queries, key_rows, value_rows, log_decay, docs)
    reach = -(-length * lax.axis_size("sp") // DOCS // length) + 1
    parts = carried(keep, give, kw, reach)
    out_weight, _ = lax.optimization_barrier((out_weight, give))
    out_weights = swapped([out_weight] * peers, "tp")
    near, factor = local(queries, key_rows, value_rows, log_decay, docs, out_gate, head_gain[None])
    residual, _ = lax.optimization_barrier((residual, near))
    streams = swapped(
        [lax.dynamic_slice_in_dim(residual, (me + s) % peers * own, own, 0) for s in range(peers)], "tp"
    )
    mixed = swapped(mix(near, factor, qf, qb, where, parts, peers), "tp")
    settled, features = settle(mixed, out_weights, streams, norm_gain, norm_bias)
    pieces = swapped([features] * peers, "tp")
    behind = lambda group: [pieces[-s % peers] for s in group]
    send = lambda part, s: lax.ppermute(part, "tp", ring("tp", s))
    direct, relayed, one, three, weights = forward(
        behind([2, 1, 3]), weights, hidden, streams=True, sizes=(own // 2, own // 2, own, own))
    direct, relayed, one, three = send(direct, 2), send(relayed, 3), send(one, 1), send(three, 3)
    own_part, = forward(behind([0]), weights, hidden)
    relayed = send(relayed, 3)
    down = [own_part, one, three, direct, relayed]
    return placed(swapped(finish(settled, down, norm_gain, norm_bias, peers), "tp"))


def solution(mesh):
    rows = ("grp", "sp")
    in_specs = (
        P(rows, "tp"), P(rows, "tp"), P(rows, "tp"), P(rows, "tp"), P(None, rows, "tp"),
        P(rows), P("tp"), P("tp", None), P(rows, "tp"), P(), P(),
        P("sp", "tp"), P("sp", "tp"), P("tp", "sp"),
    )
    return jax.shard_map(
        on_device, mesh=mesh, in_specs=in_specs, out_specs=P(rows, "tp"), check_vma=False
    )
```

```python
import functools
import jax
import jax.numpy as jnp
from jax import lax
from jax.experimental import pallas as pl
from jax.experimental.pallas import tpu as pltpu
from jax.sharding import PartitionSpec as P


DK = 32
DV = 64
DOCS = 4
EPS = 1e-06
META = 8
STREAM_MIB = 40
F32 = jnp.float32
BF = jnp.bfloat16


def iota(shape, dim):
    return lax.broadcasted_iota(jnp.int32, shape, dim)


def mm(a, b, dims=((1,), (0,))):
    return lax.dot_general(a, b, (dims, ((), ())), preferred_element_type=F32)


def partner(total, upper, h):
    n = total.shape[0]
    return jnp.where(upper, pltpu.roll(total, h, 0), pltpu.roll(total, n - h, 0))


def levels(g, r):
    n = g.shape[0]
    row = iota(g.shape, 0)
    zero = jnp.zeros_like(g)
    gi, gx, ri, rx, gt, rt = g, zero, r, zero, g, r
    h = 1
    while h < n:
        upper = (row & h) != 0
        yield h, jnp.where(upper, gi, ri), jnp.where(upper, rx, gx)
        gp, rp = partner(gt, upper, h), partner(rt, upper, h)
        gi = jnp.where(upper, gi + gp, gi)
        gx = jnp.where(upper, gx, gx + gp)
        ri = jnp.where(upper, ri, ri + rp)
        rx = jnp.where(upper, rx + rp, rx)
        gt, rt = gt + gp, rt + rp
        h *= 2
    yield n, (gi, gx, gt), (ri, rx, rt)


def rows_of(docs_row):
    n = docs_row.shape[1]
    return jnp.broadcast_to(docs_row, (128, n)).T


def head_block(kw, vw):
    return (iota((kw, vw), 0) // DK) == (iota((kw, vw), 1) // DV)


def state_of(keys, values):
    kw, vw = keys.shape[1], values.shape[1]
    full = mm(keys.astype(BF), values, ((0,), (0,)))
    full = jnp.where(head_block(kw, vw), full, 0.0)
    return functools.reduce(jnp.add, [full[a : a + DK] for a in range(0, kw, DK)])


def packed(state, passing, entry, leaving):
    vw = state.shape[1]
    wide = jnp.concatenate([passing] * (vw // passing.shape[1]), axis=1)
    line = iota((META, vw), 0)
    entry = jnp.concatenate([entry] * (vw // entry.shape[1]), axis=1)
    leaving = jnp.concatenate([leaving] * (vw // leaving.shape[1]), axis=1)
    meta = jnp.where(line == 0, wide, jnp.where(line == 1, entry, leaving))
    return jnp.concatenate([state, meta], axis=0)


def states_kernel(q_ref, k_ref, v_ref, d_ref, doc_ref, qf_ref, qb_ref, keep_ref, give_ref, docs_ref):
    n, _ = q_ref.shape
    docs = rows_of(doc_ref[...].astype(F32))
    docs_ref[...] = docs
    first, last = docs[0:1], docs[n - 1 : n]
    for h, fwd, bwd in levels(d_ref[0], d_ref[1]):
        if h == n:
            break
    gi, gx, gt = fwd
    ri, rx, rt = bwd
    q = q_ref[...].astype(F32) * DK ** (-0.5)
    k = k_ref[...].astype(F32)
    v = v_ref[...]
    qf_ref[...] = (q * jnp.exp(gi)).astype(BF)
    qb_ref[...] = (q * jnp.exp(ri)).astype(BF)
    through = jnp.where(first == last, 1.0, 0.0)
    ahead = packed(
        state_of(jnp.where(docs == last, k * jnp.exp(gx), 0.0), v),
        jnp.exp(gt[0:1]) * through, first, last)
    back = packed(
        state_of(jnp.where(docs == first, k * jnp.exp(rx), 0.0), v),
        jnp.exp(rt[0:1]) * through, last, first)
    low = on_low_core()
    keep_ref[...] = jnp.where(low, ahead, back).astype(BF)
    give_ref[...] = jnp.where(low, back, ahead).astype(BF)


def on_low_core():
    return lax.rem(lax.axis_index("sp"), 2) == 0


def spread(passing, vw):
    kw = passing.shape[1]
    place = (iota((DK, kw), 1) % DK) == iota((DK, kw), 0)
    picked = jnp.where(place, jnp.broadcast_to(passing, (DK, kw)), 0.0)
    return mm(picked.astype(BF), jnp.where(head_block(kw, vw), 1.0, 0.0).astype(BF))


def chained(links, kw):
    line = lambda a, j: a[DK + j : DK + j + 1]
    vw = links[0].shape[1]
    state, passing = links[-1][:DK], line(links[-1], 0)[:, :kw]
    for near, far in reversed(list(zip(links[:-1], links[1:]))):
        through = (line(near, 0) * jnp.where(line(near, 1) == line(far, 2), 1.0, 0.0))[:, :kw]
        state = near[:DK] + spread(through, vw) * state
        passing = passing * through
    return packed(state, passing, line(links[-1], 1)[:, :kw], line(links[0], 2)[:, :kw])


def pair_kernel(keep_ref, came_ref, out_ref, *, kw):
    out_ref[...] = chained([came_ref[...].astype(F32), keep_ref[...].astype(F32)], kw).astype(BF)


def entering_kernel(keep_ref, *refs, kw):
    out_ref, give_ref = refs[-2:]
    incoming = chained([ref[...].astype(F32) for ref in refs[:-2]], kw)
    out_ref[...] = incoming.astype(BF)
    give_ref[...] = chained([keep_ref[...].astype(F32), incoming], kw).astype(BF)


def local_kernel(q_ref, k_ref, v_ref, d_ref, doc_ref, gate_ref, gain_ref, out_ref, factor_ref, qe_ref, ke_ref):
    n, kw = q_ref.shape
    vw = v_ref.shape[1]
    half = n // 2
    gate = gate_ref[...].astype(F32)
    factor_ref[...] = gain_ref[...] * (gate / (1.0 + jnp.exp(-gate)))
    heads = kw // DK
    q = q_ref[...].astype(F32) * DK ** (-0.5)
    k = k_ref[...].astype(F32)
    hs = []
    for h, eq, ek in levels(d_ref[0], d_ref[1]):
        if h < n:
            qe_ref[len(hs)] = (q * jnp.exp(eq)).astype(BF)
            ke_ref[len(hs)] = (k * jnp.exp(ek)).astype(BF)
            hs.append(h)
    drow = doc_ref[...].astype(F32)
    dcol = rows_of(drow)
    v = v_ref[...]
    lane = iota((half, kw), 1) // DK
    olane = iota((half, vw), 1) // DV
    apart = iota((half, half), 0) ^ iota((half, half), 1)
    ones = jnp.where(head_block(kw, vw), 2.0, 0.0).astype(BF)
    same = mm((q * k).astype(BF), ones) * v.astype(F32)
    for t in range(2):
        mine = slice(t * half, (t + 1) * half)
        other = slice((1 - t) * half, (2 - t) * half)
        ok_in = (dcol[mine] == drow[:, mine]) & (apart != 0)
        ok_off = dcol[mine] == drow[:, other]
        acc = same[mine]
        for head in range(heads):
            own = lane == head
            score = None
            for l, h in enumerate(hs[:-1]):
                prod = mm(jnp.where(own, qe_ref[l, mine], 0), ke_ref[l, mine], ((1,), (1,)))
                score = prod if score is None else jnp.where(apart >= h, prod, score)
            off = mm(jnp.where(own, qe_ref[len(hs) - 1, mine], 0), ke_ref[len(hs) - 1, other], ((1,), (1,)))
            score = jnp.where(ok_in, score, 0.0).astype(BF)
            off = jnp.where(ok_off, off, 0.0).astype(BF)
            res = mm(score, v[mine]) + mm(off, v[other])
            acc = acc + jnp.where(olane == head, res, 0.0)
        out_ref[mine] = acc


def mix_kernel(near_ref, factor_ref, qf_ref, qb_ref, docs_ref, mine_ref, other_ref, *outs):
    _, kw = qf_ref.shape
    vw = near_ref.shape[1]
    docs = docs_ref[...]
    out = near_ref[...]
    block = head_block(kw, vw)
    mine, other, low = mine_ref[...].astype(F32), other_ref[...].astype(F32), on_low_core()
    for q_ref, link in ((qf_ref, jnp.where(low, mine, other)), (qb_ref, jnp.where(low, other, mine))):
        state, leaving = link[:DK], link[DK + 2 : DK + 3]
        wide = jnp.where(block, jnp.concatenate([state] * (kw // DK), axis=0), 0.0)
        reach = jnp.where(docs[:, :kw] == leaving[:, :kw], q_ref[...], 0)
        out = out + mm(reach, wide.astype(BF))
    square = out * out
    high = square.astype(BF)
    low = (square - high.astype(F32)).astype(BF)
    mean = jnp.where((iota((vw, vw), 0) // DV) == (iota((vw, vw), 1) // DV), 1.0 / DV, 0.0).astype(BF)
    power = mm(high, mean) + mm(low, mean)
    all_ref = outs[-1]
    all_ref[...] = (out * lax.rsqrt(power + EPS) * factor_ref[...]).astype(BF)
    for s, part in enumerate(outs[:-1]):
        part[...] = all_ref[place(s, part.shape[0])]


SDS = jax.ShapeDtypeStruct
VMEM = pl.BlockSpec(memory_space=pltpu.VMEM)
ANY = pl.BlockSpec(memory_space=pl.ANY)


def call(kernel, outs, args, scratch=(), flops=1 << 26, mib=8, far=False):
    return pl.pallas_call(
        kernel, out_shape=outs, scratch_shapes=scratch,
        in_specs=[VMEM] * (len(args) - far) + [ANY] * far,
        out_specs=jax.tree.map(lambda _: VMEM, outs),
        cost_estimate=pl.CostEstimate(flops=flops, bytes_accessed=1 << 20, transcendentals=1 << 17),
        compiler_params=pltpu.CompilerParams(vmem_limit_bytes=mib << 20),
    )(*args)


def states(q, k, v, d, doc):
    n, kw = q.shape
    vw = v.shape[1]
    outs = (SDS((n, kw), BF),) * 2 + (SDS((DK + META, vw), BF),) * 2
    return call(states_kernel, outs + (SDS((n, 128), F32),), (q, k, v, d, doc), mib=62)


def pair(keep, came, kw):
    return call(functools.partial(pair_kernel, kw=kw), SDS(keep.shape, BF), (keep, came))


def entering(keep, links, kw):
    return call(functools.partial(entering_kernel, kw=kw), (SDS(keep.shape, BF),) * 2, (keep, *links))


def local(q, k, v, d, doc, gate, gain):
    n, kw = q.shape
    vw = v.shape[1]
    scratch = (pltpu.VMEM((n.bit_length() - 1, n, kw), BF),) * 2
    return call(local_kernel, (SDS((n, vw), F32),) * 2, (q, k, v, d, doc, gate, gain), scratch, flops=1 << 29, mib=62)


def mix(near, factor, qf, qb, docs, parts, peers):
    n, vw = near.shape
    return call(mix_kernel, (SDS((n // peers, vw), BF),) * peers, (near, factor, qf, qb, docs, *parts),
                scratch=(pltpu.VMEM((n, vw), BF),), mib=62)


def place(step, width):
    peers = lax.axis_size("tp")
    number = lax.rem(lax.axis_index("tp") + step + peers, peers)
    return pl.ds(pl.multiple_of(number * width, width), width)


def layer_norm(stream, gain, bias):
    width = stream.shape[1]
    middle = jnp.sum(stream, axis=1, keepdims=True) / width
    offset = stream - middle
    spread = jnp.sum(offset * offset, axis=1, keepdims=True) / width
    return offset * lax.rsqrt(spread + EPS) * gain + bias


def settle_kernel(*refs, peers):
    mixed, weights, residual = (refs[j * peers : (j + 1) * peers] for j in range(3))
    gain_ref, bias_ref, settled_ref, features_ref, stream_ref = refs[3 * peers :]
    for s in range(peers):
        width = residual[s].shape[1]
        stream_ref[:, place(-s, width)] = residual[s][...].astype(F32)
    stream = stream_ref[...]
    for s in range(peers):
        stream = stream + mm(mixed[s][...], weights[s][...]).astype(BF).astype(F32)
    settled = layer_norm(stream, gain_ref[0:1], bias_ref[0:1])
    settled_ref[...] = settled
    features_ref[...] = settled.astype(BF)


def settle(mixed, weights, residual, gain, bias):
    peers = len(mixed)
    rows, width = mixed[0].shape[0], weights[0].shape[1]
    args = (*mixed, *weights, *residual, gain, bias)
    return call(functools.partial(settle_kernel, peers=peers), (SDS((rows, width), F32), SDS((rows, width), BF)),
                args, (pltpu.VMEM((rows, width), F32),), flops=1 << 28, mib=12)


def forward_kernel(*refs, count, hidden, cut, streams):
    pieces, w_ref, down, inner_ref = refs[:count], refs[count], refs[count + 1 : 2 * count + 1], refs[-1]
    n, full = pieces[0].shape
    steps = hidden // cut
    if streams:
        source, w_ref, inner_ref, sem = w_ref, *refs[-3:]
        spans = [(slice(0, full), slice(part * hidden + j * cut, part * hidden + (j + 1) * cut))
                 for j in range(steps) for part in range(2)]
        spans += [(slice(o, o + full // 2), slice(2 * hidden, 3 * hidden)) for o in range(0, full, full // 2)]
        copies = [pltpu.make_async_copy(source.at[span], w_ref.at[span], sem.at[k]) for k, span in enumerate(spans)]
        for copy in copies:
            copy.start()
    ready = lambda k: copies[k].wait() if streams else None
    x = jnp.concatenate([piece[...] for piece in pieces], axis=0) if count > 1 else pieces[0][...]
    for j in range(steps):
        a, b = j * cut, (j + 1) * cut
        ready(2 * j)
        gate = mm(x, w_ref[:, a:b])
        ready(2 * j + 1)
        up = mm(x, w_ref[:, hidden + a : hidden + b])
        inner_ref[:, a:b] = (gate / (1.0 + jnp.exp(-gate)) * up).astype(BF)
    for o in range(2):
        rows = slice(o * full // 2, (o + 1) * full // 2)
        ready(2 * steps + o)
        total = mm(inner_ref[...], w_ref[rows, 2 * hidden :], ((1,), (1,))).astype(BF)
        for s in range(count):
            down[s][:, rows] = total[s * n : (s + 1) * n]


def forward(pieces, weights, hidden, streams=False, cut=384):
    count = len(pieces)
    n, full = pieces[0].shape
    outs = (SDS((n, full), BF),) * count
    scratch = (pltpu.VMEM((count * n, hidden), BF),)
    if streams:
        outs += (SDS(weights.shape, BF),)
        scratch += (pltpu.SemaphoreType.DMA((2 * hidden // cut + 2,)),)
    return call(
        functools.partial(forward_kernel, count=count, hidden=hidden, cut=cut, streams=streams),
        outs, (*pieces, weights), scratch, flops=6 * count * n * full * hidden,
        mib=STREAM_MIB if streams else 8, far=streams)


def finish_kernel(settled_ref, *refs, peers):
    down = refs[:peers]
    gain_ref, bias_ref = refs[peers : peers + 2]
    outs, all_ref = refs[peers + 2 : -1], refs[-1]
    total = down[0][...].astype(F32)
    for s in range(1, peers):
        total = total + down[s][...].astype(F32)
    all_ref[...] = layer_norm(settled_ref[...] + 0.5 * total, gain_ref[1:2], bias_ref[1:2])
    for s in range(peers):
        outs[s][...] = all_ref[:, place(s, outs[s].shape[1])].astype(BF)


def finish(settled, down, gain, bias):
    peers = len(down)
    n, full = settled.shape
    return call(functools.partial(finish_kernel, peers=peers), (SDS((n, full // peers), BF),) * peers,
                (settled, *down, gain, bias), (pltpu.VMEM((n, full), F32),))


def placed_kernel(*refs):
    for s, part in enumerate(refs[:-1]):
        refs[-1][place(-s, part.shape[0])] = part[...]


def placed(parts):
    n, width = parts[0].shape
    return call(placed_kernel, SDS((len(parts) * n, width), BF), parts)


def ring(axis, step):
    peers = lax.axis_size(axis)
    return [(i, (i + step) % peers) for i in range(peers)]


def across(step):
    peers = lax.axis_size("sp")
    moves = [(i, i + 2 * step if i % 2 == 0 else i - 2 * step) for i in range(peers)]
    return [(i, j) for i, j in moves if 0 <= j < peers]


def other_core(x):
    return lax.ppermute(x, "sp", [(i, i ^ 1) for i in range(lax.axis_size("sp"))])


def carried(keep, give, kw, reach):
    whole = pair(keep, other_core(give), kw)
    links = [lax.ppermute(whole, "sp", across(step)) for step in range(1, -(-reach // 2) + 1)]
    mine, give = entering(keep, links, kw)
    return mine, other_core(give)


def from_peers(parts, axis):
    return [lax.ppermute(parts[s], axis, ring(axis, s)) for s in range(1, len(parts))]


def swapped(parts, axis):
    return [parts[0]] + from_peers(parts, axis)


def on_device(
    queries, key_rows, value_rows, out_gate, log_decay, doc_ids, head_gain, out_weight,
    residual, norm_gain, norm_bias, gate_weight, up_weight, down_weight,
):
    peers, me = lax.axis_size("tp"), lax.axis_index("tp")
    length, kw = queries.shape
    hidden = gate_weight.shape[1]
    own = length // peers
    weights = lax.all_gather(
        jnp.concatenate([gate_weight, up_weight, down_weight.T], axis=1), "sp", axis=0, tiled=True
    )
    docs = doc_ids[None]
    qf, qb, keep, give, where = states(queries, key_rows, value_rows, log_decay, docs)
    reach = -(-length * lax.axis_size("sp") // DOCS // length) + 1
    parts = carried(keep, give, kw, reach)
    out_weight, _ = lax.optimization_barrier((out_weight, give))
    out_weights = swapped([out_weight] * peers, "tp")
    near, factor = local(queries, key_rows, value_rows, log_decay, docs, out_gate, head_gain[None])
    residual, _ = lax.optimization_barrier((residual, near))
    streams = swapped(
        [lax.dynamic_slice_in_dim(residual, (me + s) % peers * own, own, 0) for s in range(peers)], "tp"
    )
    mixed = swapped(mix(near, factor, qf, qb, where, parts, peers), "tp")
    settled, features = settle(mixed, out_weights, streams, norm_gain, norm_bias)
    pieces = swapped([features] * peers, "tp")
    behind = lambda group: [pieces[-s % peers] for s in group]
    send = lambda part, s: lax.ppermute(part, "tp", ring("tp", s))
    two, one, three, weights = forward(behind([2, 1, 3]), weights, hidden, streams=True)
    two = send(two, 2)
    one, three = send(one, 1), send(three, 3)
    own_part, = forward(behind([0]), weights, hidden)
    return placed(swapped(finish(settled, [own_part, one, two, three], norm_gain, norm_bias), "tp"))


def solution(mesh):
    rows = ("grp", "sp")
    in_specs = (
        P(rows, "tp"), P(rows, "tp"), P(rows, "tp"), P(rows, "tp"), P(None, rows, "tp"),
        P(rows), P("tp"), P("tp", None), P(rows, "tp"), P(), P(),
        P("sp", "tp"), P("sp", "tp"), P("tp", "sp"),
    )
    return jax.shard_map(
        on_device, mesh=mesh, in_specs=in_specs, out_specs=P(rows, "tp"), check_vma=False
    )
```

```python
import functools
import jax
import jax.numpy as jnp
from jax import lax
from jax.experimental import pallas as pl
from jax.experimental.pallas import tpu as pltpu
from jax.sharding import PartitionSpec as P


DK = 32
DV = 64
DOCS = 4
EPS = 1e-06
META = 8
STREAM_MIB = 40
F32 = jnp.float32
BF = jnp.bfloat16


def iota(shape, dim):
    return lax.broadcasted_iota(jnp.int32, shape, dim)


def mm(a, b, dims=((1,), (0,))):
    return lax.dot_general(a, b, (dims, ((), ())), preferred_element_type=F32)


def partner(total, upper, h):
    n = total.shape[0]
    return jnp.where(upper, pltpu.roll(total, h, 0), pltpu.roll(total, n - h, 0))


def levels(g, r):
    n = g.shape[0]
    row = iota(g.shape, 0)
    zero = jnp.zeros_like(g)
    gi, gx, ri, rx, gt, rt = g, zero, r, zero, g, r
    h = 1
    while h < n:
        upper = (row & h) != 0
        yield h, jnp.where(upper, gi, ri), jnp.where(upper, rx, gx)
        gp, rp = partner(gt, upper, h), partner(rt, upper, h)
        gi = jnp.where(upper, gi + gp, gi)
        gx = jnp.where(upper, gx, gx + gp)
        ri = jnp.where(upper, ri, ri + rp)
        rx = jnp.where(upper, rx + rp, rx)
        gt, rt = gt + gp, rt + rp
        h *= 2
    yield n, (gi, gx, gt), (ri, rx, rt)


def rows_of(docs_row):
    n = docs_row.shape[1]
    return jnp.broadcast_to(docs_row, (128, n)).T


def head_block(kw, vw):
    return (iota((kw, vw), 0) // DK) == (iota((kw, vw), 1) // DV)


def state_of(keys, values):
    kw, vw = keys.shape[1], values.shape[1]
    full = mm(keys.astype(BF), values, ((0,), (0,)))
    full = jnp.where(head_block(kw, vw), full, 0.0)
    return functools.reduce(jnp.add, [full[a : a + DK] for a in range(0, kw, DK)])


def packed(state, passing, entry, leaving):
    vw = state.shape[1]
    wide = jnp.concatenate([passing] * (vw // passing.shape[1]), axis=1)
    line = iota((META, vw), 0)
    entry = jnp.concatenate([entry] * (vw // entry.shape[1]), axis=1)
    leaving = jnp.concatenate([leaving] * (vw // leaving.shape[1]), axis=1)
    meta = jnp.where(line == 0, wide, jnp.where(line == 1, entry, leaving))
    return jnp.concatenate([state, meta], axis=0)


def states_kernel(q_ref, k_ref, v_ref, d_ref, doc_ref, qf_ref, qb_ref, keep_ref, give_ref, docs_ref):
    n, _ = q_ref.shape
    docs = rows_of(doc_ref[...].astype(F32))
    docs_ref[...] = docs
    first, last = docs[0:1], docs[n - 1 : n]
    for h, fwd, bwd in levels(d_ref[0], d_ref[1]):
        if h == n:
            break
    gi, gx, gt = fwd
    ri, rx, rt = bwd
    q = q_ref[...].astype(F32) * DK ** (-0.5)
    k = k_ref[...].astype(F32)
    v = v_ref[...]
    qf_ref[...] = (q * jnp.exp(gi)).astype(BF)
    qb_ref[...] = (q * jnp.exp(ri)).astype(BF)
    through = jnp.where(first == last, 1.0, 0.0)
    ahead = packed(
        state_of(jnp.where(docs == last, k * jnp.exp(gx), 0.0), v),
        jnp.exp(gt[0:1]) * through, first, last)
    back = packed(
        state_of(jnp.where(docs == first, k * jnp.exp(rx), 0.0), v),
        jnp.exp(rt[0:1]) * through, last, first)
    low = on_low_core()
    keep_ref[...] = jnp.where(low, ahead, back).astype(BF)
    give_ref[...] = jnp.where(low, back, ahead).astype(BF)


def on_low_core():
    return lax.rem(lax.axis_index("sp"), 2) == 0


def spread(passing, vw):
    kw = passing.shape[1]
    place = (iota((DK, kw), 1) % DK) == iota((DK, kw), 0)
    picked = jnp.where(place, jnp.broadcast_to(passing, (DK, kw)), 0.0)
    return mm(picked.astype(BF), jnp.where(head_block(kw, vw), 1.0, 0.0).astype(BF))


def chained(links, kw):
    line = lambda a, j: a[DK + j : DK + j + 1]
    vw = links[0].shape[1]
    state, passing = links[-1][:DK], line(links[-1], 0)[:, :kw]
    for near, far in reversed(list(zip(links[:-1], links[1:]))):
        through = (line(near, 0) * jnp.where(line(near, 1) == line(far, 2), 1.0, 0.0))[:, :kw]
        state = near[:DK] + spread(through, vw) * state
        passing = passing * through
    return packed(state, passing, line(links[-1], 1)[:, :kw], line(links[0], 2)[:, :kw])


def pair_kernel(keep_ref, came_ref, out_ref, *, kw):
    out_ref[...] = chained([came_ref[...].astype(F32), keep_ref[...].astype(F32)], kw).astype(BF)


def entering_kernel(keep_ref, *refs, kw):
    out_ref, give_ref = refs[-2:]
    incoming = chained([ref[...].astype(F32) for ref in refs[:-2]], kw)
    out_ref[...] = incoming.astype(BF)
    give_ref[...] = chained([keep_ref[...].astype(F32), incoming], kw).astype(BF)


def local_kernel(q_ref, k_ref, v_ref, d_ref, doc_ref, gate_ref, gain_ref, out_ref, factor_ref, qe_ref, ke_ref):
    n, kw = q_ref.shape
    vw = v_ref.shape[1]
    half = n // 2
    gate = gate_ref[...].astype(F32)
    factor_ref[...] = gain_ref[...] * (gate / (1.0 + jnp.exp(-gate)))
    heads = kw // DK
    q = q_ref[...].astype(F32) * DK ** (-0.5)
    k = k_ref[...].astype(F32)
    hs = []
    for h, eq, ek in levels(d_ref[0], d_ref[1]):
        if h < n:
            qe_ref[len(hs)] = (q * jnp.exp(eq)).astype(BF)
            ke_ref[len(hs)] = (k * jnp.exp(ek)).astype(BF)
            hs.append(h)
    drow = doc_ref[...].astype(F32)
    dcol = rows_of(drow)
    v = v_ref[...]
    lane = iota((half, kw), 1) // DK
    olane = iota((half, vw), 1) // DV
    apart = iota((half, half), 0) ^ iota((half, half), 1)
    ones = jnp.where(head_block(kw, vw), 2.0, 0.0).astype(BF)
    same = mm((q * k).astype(BF), ones) * v.astype(F32)
    for t in range(2):
        mine = slice(t * half, (t + 1) * half)
        other = slice((1 - t) * half, (2 - t) * half)
        ok_in = (dcol[mine] == drow[:, mine]) & (apart != 0)
        ok_off = dcol[mine] == drow[:, other]
        acc = same[mine]
        for head in range(heads):
            own = lane == head
            score = None
            for l, h in enumerate(hs[:-1]):
                prod = mm(jnp.where(own, qe_ref[l, mine], 0), ke_ref[l, mine], ((1,), (1,)))
                score = prod if score is None else jnp.where(apart >= h, prod, score)
            off = mm(jnp.where(own, qe_ref[len(hs) - 1, mine], 0), ke_ref[len(hs) - 1, other], ((1,), (1,)))
            score = jnp.where(ok_in, score, 0.0).astype(BF)
            off = jnp.where(ok_off, off, 0.0).astype(BF)
            res = mm(score, v[mine]) + mm(off, v[other])
            acc = acc + jnp.where(olane == head, res, 0.0)
        out_ref[mine] = acc


def mix_kernel(near_ref, factor_ref, qf_ref, qb_ref, docs_ref, mine_ref, other_ref, *outs):
    _, kw = qf_ref.shape
    vw = near_ref.shape[1]
    docs = docs_ref[...]
    out = near_ref[...]
    block = head_block(kw, vw)
    mine, other, low = mine_ref[...].astype(F32), other_ref[...].astype(F32), on_low_core()
    for q_ref, link in ((qf_ref, jnp.where(low, mine, other)), (qb_ref, jnp.where(low, other, mine))):
        state, leaving = link[:DK], link[DK + 2 : DK + 3]
        wide = jnp.where(block, jnp.concatenate([state] * (kw // DK), axis=0), 0.0)
        reach = jnp.where(docs[:, :kw] == leaving[:, :kw], q_ref[...], 0)
        out = out + mm(reach, wide.astype(BF))
    square = out * out
    high = square.astype(BF)
    low = (square - high.astype(F32)).astype(BF)
    mean = jnp.where((iota((vw, vw), 0) // DV) == (iota((vw, vw), 1) // DV), 1.0 / DV, 0.0).astype(BF)
    power = mm(high, mean) + mm(low, mean)
    all_ref = outs[-1]
    all_ref[...] = (out * lax.rsqrt(power + EPS) * factor_ref[...]).astype(BF)
    for s, part in enumerate(outs[:-1]):
        part[...] = all_ref[place(s, part.shape[0])]


SDS = jax.ShapeDtypeStruct
VMEM = pl.BlockSpec(memory_space=pltpu.VMEM)
ANY = pl.BlockSpec(memory_space=pl.ANY)


def call(kernel, outs, args, scratch=(), flops=1 << 26, mib=8, far=False):
    return pl.pallas_call(
        kernel, out_shape=outs, scratch_shapes=scratch,
        in_specs=[VMEM] * (len(args) - far) + [ANY] * far,
        out_specs=jax.tree.map(lambda _: VMEM, outs),
        cost_estimate=pl.CostEstimate(flops=flops, bytes_accessed=1 << 20, transcendentals=1 << 17),
        compiler_params=pltpu.CompilerParams(vmem_limit_bytes=mib << 20),
    )(*args)


def states(q, k, v, d, doc):
    n, kw = q.shape
    vw = v.shape[1]
    outs = (SDS((n, kw), BF),) * 2 + (SDS((DK + META, vw), BF),) * 2
    return call(states_kernel, outs + (SDS((n, 128), F32),), (q, k, v, d, doc), mib=62)


def pair(keep, came, kw):
    return call(functools.partial(pair_kernel, kw=kw), SDS(keep.shape, BF), (keep, came))


def entering(keep, links, kw):
    return call(functools.partial(entering_kernel, kw=kw), (SDS(keep.shape, BF),) * 2, (keep, *links))


def local(q, k, v, d, doc, gate, gain):
    n, kw = q.shape
    vw = v.shape[1]
    scratch = (pltpu.VMEM((n.bit_length() - 1, n, kw), BF),) * 2
    return call(local_kernel, (SDS((n, vw), F32),) * 2, (q, k, v, d, doc, gate, gain), scratch, flops=1 << 29, mib=62)


def mix(near, factor, qf, qb, docs, parts, peers):
    n, vw = near.shape
    return call(mix_kernel, (SDS((n // peers, vw), BF),) * peers, (near, factor, qf, qb, docs, *parts),
                scratch=(pltpu.VMEM((n, vw), BF),), mib=62)


def place(step, width):
    peers = lax.axis_size("tp")
    number = lax.rem(lax.axis_index("tp") + step + peers, peers)
    return pl.ds(pl.multiple_of(number * width, width), width)


def layer_norm(stream, gain, bias):
    width = stream.shape[1]
    middle = jnp.sum(stream, axis=1, keepdims=True) / width
    offset = stream - middle
    spread = jnp.sum(offset * offset, axis=1, keepdims=True) / width
    return offset * lax.rsqrt(spread + EPS) * gain + bias


def settle_kernel(*refs, peers):
    mixed, weights, residual = (refs[j * peers : (j + 1) * peers] for j in range(3))
    gain_ref, bias_ref, settled_ref, features_ref, stream_ref = refs[3 * peers :]
    for s in range(peers):
        width = residual[s].shape[1]
        stream_ref[:, place(-s, width)] = residual[s][...].astype(F32)
    stream = stream_ref[...]
    for s in range(peers):
        stream = stream + mm(mixed[s][...], weights[s][...]).astype(BF).astype(F32)
    settled = layer_norm(stream, gain_ref[0:1], bias_ref[0:1])
    settled_ref[...] = settled
    features_ref[...] = settled.astype(BF)


def settle(mixed, weights, residual, gain, bias):
    peers = len(mixed)
    rows, width = mixed[0].shape[0], weights[0].shape[1]
    args = (*mixed, *weights, *residual, gain, bias)
    return call(functools.partial(settle_kernel, peers=peers), (SDS((rows, width), F32), SDS((rows, width), BF)),
                args, (pltpu.VMEM((rows, width), F32),), flops=1 << 28, mib=12)


def forward_kernel(*refs, count, hidden, cut, streams):
    pieces, w_ref, down, inner_ref = refs[:count], refs[count], refs[count + 1 : 2 * count + 1], refs[-1]
    n, full = pieces[0].shape
    steps = hidden // cut
    if streams:
        source, w_ref, inner_ref, sem = w_ref, *refs[-3:]
        spans = [(slice(0, full), slice(part * hidden + j * cut, part * hidden + (j + 1) * cut))
                 for j in range(steps) for part in range(2)]
        spans += [(slice(o, o + full // 2), slice(2 * hidden, 3 * hidden)) for o in range(0, full, full // 2)]
        copies = [pltpu.make_async_copy(source.at[span], w_ref.at[span], sem.at[k]) for k, span in enumerate(spans)]
        for copy in copies:
            copy.start()
    ready = lambda k: copies[k].wait() if streams else None
    x = jnp.concatenate([piece[...] for piece in pieces], axis=0) if count > 1 else pieces[0][...]
    for j in range(steps):
        a, b = j * cut, (j + 1) * cut
        ready(2 * j)
        gate = mm(x, w_ref[:, a:b])
        ready(2 * j + 1)
        up = mm(x, w_ref[:, hidden + a : hidden + b])
        inner_ref[:, a:b] = (gate / (1.0 + jnp.exp(-gate)) * up).astype(BF)
    for o in range(2):
        rows = slice(o * full // 2, (o + 1) * full // 2)
        ready(2 * steps + o)
        total = mm(inner_ref[...], w_ref[rows, 2 * hidden :], ((1,), (1,))).astype(BF)
        for s in range(count):
            down[s][:, rows] = total[s * n : (s + 1) * n]


def forward(pieces, weights, hidden, streams=False, cut=384):
    count = len(pieces)
    n, full = pieces[0].shape
    outs = (SDS((n, full), BF),) * count
    scratch = (pltpu.VMEM((count * n, hidden), BF),)
    if streams:
        outs += (SDS(weights.shape, BF),)
        scratch += (pltpu.SemaphoreType.DMA((2 * hidden // cut + 2,)),)
    return call(
        functools.partial(forward_kernel, count=count, hidden=hidden, cut=cut, streams=streams),
        outs, (*pieces, weights), scratch, flops=6 * count * n * full * hidden,
        mib=STREAM_MIB if streams else 8, far=streams)


def finish_kernel(settled_ref, *refs, peers):
    down = refs[:peers]
    gain_ref, bias_ref = refs[peers : peers + 2]
    outs, all_ref = refs[peers + 2 : -1], refs[-1]
    total = down[0][...].astype(F32)
    for s in range(1, peers):
        total = total + down[s][...].astype(F32)
    all_ref[...] = layer_norm(settled_ref[...] + 0.5 * total, gain_ref[1:2], bias_ref[1:2])
    for s in range(peers):
        outs[s][...] = all_ref[:, place(s, outs[s].shape[1])].astype(BF)


def finish(settled, down, gain, bias):
    peers = len(down)
    n, full = settled.shape
    return call(functools.partial(finish_kernel, peers=peers), (SDS((n, full // peers), BF),) * peers,
                (settled, *down, gain, bias), (pltpu.VMEM((n, full), F32),))


def placed_kernel(*refs):
    for s, part in enumerate(refs[:-1]):
        refs[-1][place(-s, part.shape[0])] = part[...]


def placed(parts):
    n, width = parts[0].shape
    return call(placed_kernel, SDS((len(parts) * n, width), BF), parts)


def ring(axis, step):
    peers = lax.axis_size(axis)
    return [(i, (i + step) % peers) for i in range(peers)]


def across(step):
    chips = lax.axis_size("sp") // 2
    span = chips // DOCS
    reach = lambda behind: behind + 1 if behind else span + 1
    up = [(2 * (chip - step), 2 * chip) for chip in range(step, chips) if step <= reach(chip % span)]
    down = [(2 * (chip + step) + 1, 2 * chip + 1) for chip in range(chips - step) if step <= reach(span - 1 - chip % span)]
    return up + down


def other_core(x):
    return lax.ppermute(x, "sp", [(i, i ^ 1) for i in range(lax.axis_size("sp"))])


def carried(keep, give, kw, reach):
    whole = pair(keep, other_core(give), kw)
    links = [lax.ppermute(whole, "sp", across(step)) for step in range(1, -(-reach // 2) + 1)]
    mine, give = entering(keep, links, kw)
    return mine, other_core(give)


def from_peers(parts, axis):
    return [lax.ppermute(parts[s], axis, ring(axis, s)) for s in range(1, len(parts))]


def swapped(parts, axis):
    return [parts[0]] + from_peers(parts, axis)


def on_device(
    queries, key_rows, value_rows, out_gate, log_decay, doc_ids, head_gain, out_weight,
    residual, norm_gain, norm_bias, gate_weight, up_weight, down_weight,
):
    peers, me = lax.axis_size("tp"), lax.axis_index("tp")
    length, kw = queries.shape
    hidden = gate_weight.shape[1]
    own = length // peers
    weights = lax.all_gather(
        jnp.concatenate([gate_weight, up_weight, down_weight.T], axis=1), "sp", axis=0, tiled=True
    )
    docs = doc_ids[None]
    qf, qb, keep, give, where = states(queries, key_rows, value_rows, log_decay, docs)
    reach = -(-length * lax.axis_size("sp") // DOCS // length) + 1
    parts = carried(keep, give, kw, reach)
    out_weight, _ = lax.optimization_barrier((out_weight, give))
    out_weights = swapped([out_weight] * peers, "tp")
    near, factor = local(queries, key_rows, value_rows, log_decay, docs, out_gate, head_gain[None])
    residual, _ = lax.optimization_barrier((residual, near))
    streams = swapped(
        [lax.dynamic_slice_in_dim(residual, (me + s) % peers * own, own, 0) for s in range(peers)], "tp"
    )
    mixed = swapped(mix(near, factor, qf, qb, where, parts, peers), "tp")
    settled, features = settle(mixed, out_weights, streams, norm_gain, norm_bias)
    pieces = swapped([features] * peers, "tp")
    behind = lambda group: [pieces[-s % peers] for s in group]
    send = lambda part, s: lax.ppermute(part, "tp", ring("tp", s))
    two, one, three, weights = forward(behind([2, 1, 3]), weights, hidden, streams=True)
    two = send(two, 2)
    one, three = send(one, 1), send(three, 3)
    own_part, = forward(behind([0]), weights, hidden)
    return placed(swapped(finish(settled, [own_part, one, two, three], norm_gain, norm_bias), "tp"))


def solution(mesh):
    rows = ("grp", "sp")
    in_specs = (
        P(rows, "tp"), P(rows, "tp"), P(rows, "tp"), P(rows, "tp"), P(None, rows, "tp"),
        P(rows), P("tp"), P("tp", None), P(rows, "tp"), P(), P(),
        P("sp", "tp"), P("sp", "tp"), P("tp", "sp"),
    )
    return jax.shard_map(
        on_device, mesh=mesh, in_specs=in_specs, out_specs=P(rows, "tp"), check_vma=False
    )
```
